512 devices in a mesh: ep: 32 (over z, core), tp: 16 (over y, x).
Axes of the slice: x: 4, y: 4, z: 16, core: 2. Of those that a mesh axis runs over, the one named last changes fastest.
Arguments:
- queries: bfloat16 [12288, 2048], P('ep', 'tp'), may hold values from -6 to 6
- keys: bfloat16 [12288, 2048], P('ep', 'tp'), may hold values from -6 to 6
- values: bfloat16 [12288, 2048], P('ep', 'tp'), may hold values from -6 to 6
- key_bias: bfloat16 [12288, 16], P('ep', 'tp'), may hold values from -14 to -1.5
- moe_in: bfloat16 [4096, 2048], P(('ep', 'tp')), may hold values from -6 to 6
- norm_gain: float32 [2048], replicated, may hold values from 0.1 to 1.9
- route_ids: int32 [4096, 4], P('ep'), may hold values from 0 to 63, all different within a row; in each aligned block of 8 rows (0 to 7, 8 to 15, ...) at most 1 rows name the same one
- route_weights: float32 [4096, 4], P(('ep', 'tp')), may hold values from 0.1 to 1
- gate_weight: bfloat16 [64, 1024, 2048], P('ep', 'tp'), may hold values from -0.125 to 0.125
- up_weight: bfloat16 [64, 1024, 2048], P('ep', 'tp'), may hold values from -0.125 to 0.125
- down_weight: bfloat16 [64, 1024, 2048], P('ep', 'tp'), may hold values from -0.1875 to 0.1875
- shared_gate: bfloat16 [1024, 2048], P('tp'), may hold values from -0.125 to 0.125
- shared_up: bfloat16 [1024, 2048], P('tp'), may hold values from -0.125 to 0.125
- shared_down: bfloat16 [1024, 2048], P('tp'), may hold values from -0.1875 to 0.1875
Outputs:
- heads_out: bfloat16 [12288, 2048], P('ep', 'tp')
- moe_out: bfloat16 [4096, 2048], P(('ep', 'tp'))
The draws below stay inside these ranges and needn't reach their ends.
Inputs may be any that keep to these rules, and one draw needn't show every extreme that they name: `route_ids`: each row names 4 different experts. Among the 8 rows of one device (an aligned block of 8 rows) no expert is named more than once.
All inputs are finite; a program needn't handle non-finite values.
Results may differ from the reference program's by a relative error of at most 0.015.
Values may be sent and summed in bfloat16 or wider, within the bound.
A program may use at most 128 MiB of HBM per device.

```python
import math
import jax
import jax.numpy as jnp
import numpy as np
from jax import lax

D = 2048
HEADS = 16
HEAD_DIM = 128
FF = 1024
SFF = 1024
TOPK = 4
TOKENS1 = 12288
TOKENS2 = 4096
EXPERTS = 64
ROWS2_DEV = 8
CAP = 1
N_EP = 32
N_TP = 16


def draw_key_bias(key, part):
    kind_key, keep_key, fast_key, slow_key, fine_key = jax.random.split(jax.random.fold_in(key, 7), 5)
    keep_share = 0.5
    keeping = jax.random.uniform(kind_key, (HEADS,), jnp.float32) < keep_share
    keep_level = jnp.log(jax.random.uniform(keep_key, (HEADS,), jnp.float32, 0.2, 1.2) / TOKENS1)
    fast_level = jax.random.uniform(fast_key, (HEADS,), jnp.float32, -4.5, -3.0)
    base_level = jnp.where(keeping, keep_level, fast_level)
    slow_part = jax.random.uniform(slow_key, (TOKENS1 // 64, HEADS), jnp.float32, -0.7, 0.7)
    slow_part = jnp.repeat(slow_part, 64, axis=0)
    fine_part = jax.random.uniform(fine_key, (TOKENS1, HEADS), jnp.float32, -0.6, 0.6)
    return (base_level[None, :] + slow_part + fine_part).astype(jnp.bfloat16)


def block_scale(own_key, extent, shards, low, largest):
    loudness, own = 1.0, jax.random.fold_in(own_key, 6)
    for position, blocks in shards:
        draws = jnp.exp(jax.random.uniform(jax.random.fold_in(own, position), (blocks,), jnp.float32, low / len(shards), largest / len(shards)))
        loudness = loudness * jnp.repeat(draws, extent[position] // blocks).reshape([-1 if axis == position else 1 for axis in range(len(extent))])
    return loudness


def deal_out(stream_key, own, number, rows, amount, top, reach, slope):
    sequence = jax.random.permutation(stream_key, amount)
    heavy_load, usual = load_shares(amount, rows * top, reach, slope, True), load_shares(amount, rows * top, reach, slope, False)
    places = jnp.arange(amount)

    def named(lengths, rotation):
        used = int((lengths > 0).sum())
        fixed = max(1, used // 4)
        passed = fixed + (places - fixed + rotation * (used - fixed)) % max(1, amount - fixed)
        return jnp.zeros((amount,), jnp.int32).at[sequence[jnp.where(places < fixed, places, passed)]].set(jnp.asarray(lengths, jnp.int32))

    lengths = jnp.where(number % 4 == 0, named(heavy_load, number // 4), named(usual, number - number // 4 - 1))
    mixed = jax.random.permutation(jax.random.fold_in(own, 3), amount)
    source_of, taker = mixed[0:amount // 2 * 2:2], mixed[1:amount // 2 * 2:2]
    slack = jnp.minimum(lengths[source_of] - 1, reach - lengths[taker]) // 2
    slack = jnp.where((source_of == sequence[0]) | (taker == sequence[0]) | (lengths[taker] == 0), 0, jnp.maximum(slack, 0))
    passed = jax.random.randint(jax.random.fold_in(own, 4), (amount // 2,), 0, 1 << 20) % (slack + 1)
    lengths = lengths.at[source_of].add(-passed).at[taker].add(passed)
    members = jnp.searchsorted(jnp.cumsum(lengths), jnp.arange(rows * top), side="right").astype(jnp.int32)
    listing = members.reshape(top, rows).T
    listing = listing[jax.random.permutation(jax.random.fold_in(own, 1), rows)]
    rotation = jax.random.randint(jax.random.fold_in(own, 2), (rows, 1), 0, top)
    return jnp.take_along_axis(listing, (jnp.arange(top)[None, :] + rotation) % top, axis=1)


def load_shares(number_of, total, reach, lean, full):
    weights = [(1 << 20) // math.isqrt(grade ** lean) + 1 for grade in range(1, number_of + 1)]
    largest = reach if full else min(reach, max(-(-total // number_of), total * weights[0] // sum(weights)))
    least = 1 if total - largest >= number_of - 1 else 0
    holding, spare = [largest] + [least] * (number_of - 1), total - largest - least * (number_of - 1)
    while spare > 0:
        free = [i for i in range(1, number_of) if holding[i] < largest] or [i for i in range(1, number_of) if holding[i] < reach]
        mass, remaining = sum([weights[i] for i in free]), spare
        for i in free:
            addition = min(reach - holding[i], max(1, remaining * weights[i] // mass), spare)
            holding[i] = holding[i] + addition
            spare = spare - addition
    return np.array(holding)


def gaussian(key, dims, deviation, most, cuts=(), kind=jnp.bfloat16):
    values = jax.random.normal(key, dims, jnp.float32) * deviation
    if len(cuts) > 0:
        values = block_scale(key, dims, cuts, -0.22, 0.18) * values
    return jnp.clip(values, min=-most, max=most).astype(kind)


def setup_inputs(seed: int = 0) -> dict:
    splits = jax.random.split(jax.random.key(seed), 15)
    queries = gaussian(splits[0], (TOKENS1, HEADS * HEAD_DIM), 1.0, 6.0, ((0, 32), (1, 16)))
    keys = gaussian(splits[1], (TOKENS1, HEADS * HEAD_DIM), 1.0, 6.0, ((0, 32), (1, 16)))
    values = gaussian(splits[2], (TOKENS1, HEADS * HEAD_DIM), 1.0, 6.0, ((0, 32), (1, 16)))
    key_bias = draw_key_bias(jax.random.fold_in(splits[14], 71), 0)
    moe_in = gaussian(splits[4], (TOKENS2, D), 1.0, 6.0, ((0, 512),))
    norm_gain = jnp.clip(1.0 + 0.18 * jax.random.normal(splits[5], (D,), jnp.float32), 0.1, 1.9)
    route_ids_keys = jax.random.split(jax.random.fold_in(splits[6], 1), TOKENS2 // ROWS2_DEV)
    route_ids_turns = jax.random.permutation(jax.random.fold_in(splits[6], 3), TOKENS2 // ROWS2_DEV)
    route_ids = jax.vmap(lambda own, number: deal_out(jax.random.fold_in(splits[6], 2), own, number, ROWS2_DEV, EXPERTS, TOPK, CAP, 1))(route_ids_keys, route_ids_turns).reshape((TOKENS2, TOPK))
    route_weights = jnp.clip(0.1 + 0.9 * jax.random.uniform(splits[7], (TOKENS2, TOPK), jnp.float32) ** block_scale(splits[7], (TOKENS2, TOPK), ((0, 512),), -0.2, 0.2), 0.1, 1.0)
    gate_weight = gaussian(splits[8], (EXPERTS, FF, D), D ** -0.5, 0.125, ((0, 32), (1, 16)))
    up_weight = gaussian(splits[9], (EXPERTS, FF, D), D ** -0.5, 0.125, ((0, 32), (1, 16)))
    down_weight = gaussian(splits[10], (EXPERTS, FF, D), FF ** -0.5, 0.1875, ((0, 32), (1, 16)))
    shared_gate = gaussian(splits[11], (SFF, D), D ** -0.5, 0.125, ((0, 16),))
    shared_up = gaussian(splits[12], (SFF, D), D ** -0.5, 0.125, ((0, 16),))
    shared_down = gaussian(splits[13], (SFF, D), SFF ** -0.5, 0.1875, ((0, 16),))
    return dict(queries=queries, keys=keys, values=values, key_bias=key_bias, moe_in=moe_in, norm_gain=norm_gain, route_ids=route_ids, route_weights=route_weights, gate_weight=gate_weight, up_weight=up_weight, down_weight=down_weight, shared_gate=shared_gate, shared_up=shared_up, shared_down=shared_down)


norm_eps = 1e-05

def stick_head(q_head, k_head, v_head, b_head):
    total = q_head.shape[0]
    qblock = math.gcd(total, 512)
    scale_factor = q_head.shape[1] ** (-0.5)
    key_pos = jnp.arange(total, dtype=jnp.int32)
    bias_row = b_head.astype(jnp.float32)

    def one_block(index):
        q_rows = lax.dynamic_slice_in_dim(q_head, index * qblock, qblock, 0)
        query_pos = index * qblock + jnp.arange(qblock, dtype=jnp.int32)
        scores = jnp.dot(q_rows, k_head.T, preferred_element_type=jnp.float32) * scale_factor + bias_row[None, :]
        causal = key_pos[None, :] < query_pos[:, None]
        log_keep = jnp.where(causal, -jax.nn.softplus(scores), jnp.float32(0.0))
        between = lax.cumsum(log_keep, axis=1, reverse=True) - log_keep
        weights = jnp.where(causal, jnp.exp(jax.nn.log_sigmoid(scores) + between), jnp.float32(0.0)).astype(jnp.bfloat16)
        raw_out = jnp.dot(weights, v_head, preferred_element_type=jnp.float32)
        scaled = raw_out * lax.rsqrt(lax.optimization_barrier(jnp.mean(raw_out * raw_out, axis=1, keepdims=True)) + norm_eps)
        return scaled.astype(jnp.bfloat16)
    blocks = lax.map(one_block, jnp.arange(total // qblock, dtype=jnp.int32))
    return blocks.reshape(total, q_head.shape[1])

def per_head(packed):
    return stick_head(packed[0], packed[1], packed[2], packed[3])

def swiglu(inputs, gate, up_proj):
    gate_val = jnp.dot(inputs, gate.T, preferred_element_type=jnp.float32)
    up_val = jnp.dot(inputs, up_proj.T, preferred_element_type=jnp.float32)
    return (jax.nn.silu(gate_val) * up_val).astype(jnp.bfloat16)

def sliced_sum(hidden, down, pieces):
    count = hidden.shape[0]
    group = hidden.shape[1] // pieces
    hidden_three = hidden.astype(jnp.float32).reshape(count, pieces, group)
    down_three = down.astype(jnp.float32).reshape(pieces, group, down.shape[1])
    partial_value = jnp.einsum('rpf,pfd->rpd', hidden_three, down_three, precision=lax.Precision.HIGHEST)
    rounded = lax.optimization_barrier(partial_value.astype(jnp.bfloat16))
    return lax.optimization_barrier(jnp.sum(rounded.astype(jnp.float32), axis=1))

def reference(queries, keys, values, key_bias, moe_in, norm_gain, route_ids, route_weights, gate_weight, up_weight, down_weight, shared_gate, shared_up, shared_down):
    total, width = queries.shape
    heads = key_bias.shape[1]
    head_dim = width // heads

    def split_heads(array):
        return array.reshape(total, heads, head_dim).transpose(1, 0, 2)
    per_heads = lax.map(per_head, (split_heads(queries), split_heads(keys), split_heads(values), key_bias.T))
    heads_out = per_heads.transpose(1, 0, 2).reshape(total, width)
    as_float = moe_in.astype(jnp.float32)
    normed = (as_float * lax.rsqrt(lax.optimization_barrier(jnp.mean(as_float * as_float, axis=1, keepdims=True)) + norm_eps) * norm_gain).astype(jnp.bfloat16)
    rows_total, model_width = normed.shape
    rblock = math.gcd(rows_total, 512)

    def shared_block(block_rows):
        return sliced_sum(swiglu(block_rows, shared_gate, shared_up), shared_down, N_TP)
    shared_term = lax.map(shared_block, normed.reshape(rows_total // rblock, rblock, model_width)).reshape(rows_total, model_width)
    bound = min(TOKENS2, N_EP * N_TP * CAP)

    def one_expert(accum, packed):
        gate, up_proj, down, expert = packed
        chosen_k = route_ids == expert
        row_weight = lax.optimization_barrier(jnp.sum(jnp.where(chosen_k, route_weights, jnp.float32(0.0)), axis=1))
        chosen = jnp.any(chosen_k, axis=1)
        index = jnp.nonzero(chosen, size=bound, fill_value=0)[0].astype(jnp.int32)
        valid = jnp.arange(bound, dtype=jnp.int32) < jnp.sum(chosen.astype(jnp.int32))
        picked = normed[index]
        result = lax.optimization_barrier(sliced_sum(swiglu(picked, gate, up_proj), down, N_TP).astype(jnp.bfloat16))
        contrib = jnp.where(valid[:, None], row_weight[index][:, None] * result.astype(jnp.float32), jnp.float32(0.0))
        return (accum.at[index].add(contrib), None)
    routed, _ = lax.scan(one_expert, jnp.zeros((rows_total, model_width), jnp.float32), (gate_weight, up_weight, down_weight, jnp.arange(gate_weight.shape[0], dtype=jnp.int32)))
    moe_out = (shared_term + routed).astype(jnp.bfloat16)
    return (heads_out, moe_out)
```

```python
import functools

import jax
import jax.numpy as jnp
from jax import lax
from jax.experimental import pallas as pl
from jax.experimental.pallas import tpu as pltpu
from jax.sharding import Mesh
from jax.sharding import PartitionSpec as P

TP = ("tp_0", "tp_1")
EP_TP = ("ep", "tp_0", "tp_1")


norm_eps = 1e-05


def in_one_piece(arrays, axis, dim, along):
    widths = [a.shape[along] for a in arrays]
    both = jnp.concatenate(arrays, axis=along)
    filled = lax.all_gather(both, axis, axis=dim, tiled=True)
    return tuple(jnp.split(filled, [sum(widths[:k]) for k in range(1, len(widths))], axis=along))


def joined_along(pieces, dim):
    pieces = jnp.moveaxis(pieces, 0, dim)
    lengths = pieces.shape
    return pieces.reshape(*lengths[:dim], lengths[dim] * lengths[dim + 1], *lengths[dim + 2 :])


def from_everyone(value, axis):
    copies = jnp.broadcast_to(value, (lax.axis_size(axis), *value.shape))
    return lax.all_to_all(copies, axis, split_axis=0, concat_axis=0, tiled=True)


def gather_directly(value, axis, dim):
    return joined_along(from_everyone(value, axis), dim)


def summed_rows(terms, axes):
    so_far = terms.astype(jnp.bfloat16)
    for axis in axes:
        so_far = lax.psum_scatter(so_far, axis, scatter_dimension=0, tiled=True)
    return so_far.astype(jnp.float32)


def packed_rows(keys, values, key_bias):
    num_rows, width = keys.shape
    bias_rows = key_bias.reshape(num_rows // width, width)
    return jnp.concatenate(
        [keys, values, jnp.pad(bias_rows, ((0, 16 - bias_rows.shape[0]), (0, 0)))], axis=0
    )


def attention_kernel(scale_factor, q_ref, kv_ref, o_ref, tri, acc, later):
    num_rows, width = q_ref.shape
    chunk = 128
    me = lax.axis_index("ep")
    row_id = lax.broadcasted_iota(jnp.int32, (num_rows, num_rows + 128), 0)
    col_id = lax.broadcasted_iota(jnp.int32, (num_rows, num_rows + 128), 1)
    tri[...] = jnp.where((row_id > col_id) | (col_id >= num_rows), -1.0, 0.0).astype(jnp.bfloat16)
    acc[...] = jnp.zeros_like(acc)
    later[...] = jnp.zeros_like(later)

    def visit(block, diagonal):
        k_block = kv_ref[block, :num_rows, :]
        v_block = kv_ref[block, num_rows : 2 * num_rows, :]
        bias = kv_ref[block, 2 * num_rows : 2 * num_rows + 16, :].astype(jnp.float32)
        bias = jnp.concatenate([bias[r : r + 1] for r in range(num_rows // width)], axis=1)
        for first in range(0, num_rows, chunk):
            rows = slice(first, first + chunk)
            scores = (
                lax.dot_general(
                    q_ref[rows, :],
                    k_block,
                    (((1,), (1,)), ((), ())),
                    preferred_element_type=jnp.float32,
                )
                * scale_factor
                + bias
            )
            soft = jnp.maximum(scores, jnp.log(1.0 + jnp.exp(jnp.minimum(scores, 88.0))))
            dropped = soft
            if diagonal:
                causal = lax.broadcasted_iota(
                    jnp.int32, scores.shape, 1
                ) < first + lax.broadcasted_iota(jnp.int32, scores.shape, 0)
                dropped = jnp.where(causal, soft, 0.0)
            sums = jnp.dot(
                dropped.astype(jnp.bfloat16), tri[...], preferred_element_type=jnp.float32
            )
            carried = later[rows, :]
            between = sums[:, :num_rows] + jnp.concatenate(
                [carried] * (num_rows // width), axis=1
            )
            weights = jnp.exp(scores - soft + between)
            if diagonal:
                weights = jnp.where(causal, weights, 0.0)
            acc[rows, :] += jnp.dot(
                weights.astype(jnp.bfloat16), v_block, preferred_element_type=jnp.float32
            )
            later[rows, :] = carried + sums[:, num_rows:]

    visit(me, True)

    def earlier(count, carry):
        visit(me - 1 - count, False)
        return carry

    lax.fori_loop(0, me, earlier, 0)
    raw_out = acc[...]
    o_ref[...] = (
        raw_out * lax.rsqrt(jnp.mean(raw_out * raw_out, axis=1, keepdims=True) + norm_eps)
    ).astype(jnp.bfloat16)


def stick_half(queries, keys, values, key_bias):
    num_rows, width = queries.shape
    filled = lax.all_gather(packed_rows(keys, values, key_bias), "ep", axis=0, tiled=False)
    return pl.pallas_call(
        functools.partial(attention_kernel, width ** (-0.5)),
        out_shape=jax.ShapeDtypeStruct((num_rows, width), jnp.bfloat16),
        in_specs=[pl.BlockSpec(memory_space=pltpu.VMEM)] * 2,
        out_specs=pl.BlockSpec(memory_space=pltpu.VMEM),
        scratch_shapes=[
            pltpu.VMEM((num_rows, num_rows + 128), jnp.bfloat16),
            pltpu.VMEM((num_rows, width), jnp.float32),
            pltpu.VMEM((num_rows, 128), jnp.float32),
        ],
        compiler_params=pltpu.CompilerParams(vmem_limit_bytes=40 * 1024 * 1024),
        cost_estimate=pl.CostEstimate(
            flops=8_000_000_000, bytes_accessed=7_000_000, transcendentals=14_000_000
        ),
    )(queries, filled)


def expert_terms(
    routed, shared_rows, gate_weight, up_weight, down_weight, shared_gate, shared_up, shared_down
):
    blocks = routed.shape[0]
    width = routed.shape[3]
    gate_val = jnp.einsum("besd,efd->besf", routed, gate_weight, preferred_element_type=jnp.float32)
    up_val = jnp.einsum("besd,efd->besf", routed, up_weight, preferred_element_type=jnp.float32)
    hidden = (jax.nn.silu(gate_val) * up_val).astype(jnp.bfloat16)
    routed_out = jnp.einsum(
        "besf,efd->besd", hidden, down_weight, preferred_element_type=jnp.float32
    )
    routed_out = routed_out.reshape(blocks, -1, width)
    shared_gv = jnp.einsum(
        "nd,fd->nf", shared_rows, shared_gate, preferred_element_type=jnp.float32
    )
    shared_uv = jnp.einsum("nd,fd->nf", shared_rows, shared_up, preferred_element_type=jnp.float32)
    shared_hidden = (jax.nn.silu(shared_gv) * shared_uv).astype(jnp.bfloat16)
    shared_out = jnp.einsum(
        "nf,fd->nd", shared_hidden, shared_down, preferred_element_type=jnp.float32
    )
    shared_out = shared_out.reshape(blocks, -1, width)
    return jnp.concatenate([routed_out, shared_out], axis=1).reshape(-1, width)


def expert_half(
    moe_in,
    norm_gain,
    route_ids,
    route_weights,
    gate_weight,
    up_weight,
    down_weight,
    shared_gate,
    shared_up,
    shared_down,
):
    own_rows, width = moe_in.shape
    top_k = route_weights.shape[1]
    local_experts = gate_weight.shape[0]
    ep_count = lax.axis_size("ep")
    tp_count = lax.axis_size(TP)
    expert_count = local_experts * ep_count
    capacity = max(1, 2 * own_rows * tp_count * top_k // (tp_count * expert_count))
    slot_total = local_experts * ep_count * capacity
    term_rows = slot_total + own_rows
    tp_index = lax.axis_index(TP)
    as_float = moe_in.astype(jnp.float32)
    normed = (
        as_float
        * lax.rsqrt(jnp.mean(as_float * as_float, axis=1, keepdims=True) + norm_eps)
        * norm_gain
    ).astype(jnp.bfloat16)
    flat_ids = route_ids.reshape(tp_count, own_rows * top_k)
    one_hot = (flat_ids[:, :, None] == jnp.arange(expert_count, dtype=jnp.int32)).astype(jnp.int32)
    ranks = jnp.sum((jnp.cumsum(one_hot, axis=1) - one_hot) * one_hot, axis=2)
    dest_ep = flat_ids // local_experts
    local_index = flat_ids % local_experts
    local_slot = local_index * (ep_count * capacity) + dest_ep * capacity + ranks
    own_slots = lax.dynamic_index_in_dim(local_slot, tp_index, 0, keepdims=False)
    row_of = jnp.arange(own_rows * top_k, dtype=jnp.int32) // top_k
    source_row = jnp.full((slot_total,), own_rows, jnp.int32).at[own_slots].set(row_of)
    outgoing = jnp.take(normed, source_row, axis=0, mode="fill", fill_value=0)
    outgoing = outgoing.reshape(local_experts, ep_count, capacity, width)
    arrived = lax.all_to_all(outgoing, "ep", split_axis=1, concat_axis=1, tiled=True)
    pooled = gather_directly(
        jnp.concatenate([arrived.reshape(slot_total, width), normed], axis=0), TP, 0
    )
    blocks = term_rows * lax.axis_size(TP) // term_rows
    portion = pooled.reshape(blocks, term_rows, width)
    routed = portion[:, :slot_total].reshape(blocks, local_experts, ep_count * capacity, width)
    shared_rows = portion[:, slot_total:].reshape(blocks * own_rows, width)
    summed = summed_rows(
        expert_terms(
            routed,
            shared_rows,
            gate_weight,
            up_weight,
            down_weight,
            shared_gate,
            shared_up,
            shared_down,
        ),
        TP,
    )
    slot_out = (
        summed[:slot_total].astype(jnp.bfloat16).reshape(local_experts, ep_count, capacity, width)
    )
    returned = lax.all_to_all(slot_out, "ep", split_axis=1, concat_axis=1, tiled=True).reshape(
        slot_total, width
    )
    picked = (
        jnp.take(returned, own_slots, axis=0).astype(jnp.float32).reshape(own_rows, top_k, width)
    )
    combined = summed[slot_total:] + jnp.sum(picked * route_weights[:, :, None], axis=1)
    return combined.astype(jnp.bfloat16)


def shards(
    queries,
    keys,
    values,
    key_bias,
    moe_in,
    norm_gain,
    route_ids,
    route_weights,
    gate_weight,
    up_weight,
    down_weight,
    shared_gate,
    shared_up,
    shared_down,
):
    heads_out = stick_half(queries, keys, values, key_bias)
    moe_out = expert_half(
        moe_in,
        norm_gain,
        route_ids,
        route_weights,
        gate_weight,
        up_weight,
        down_weight,
        shared_gate,
        shared_up,
        shared_down,
    )
    return (heads_out, moe_out)


def solution(mesh):
    split = Mesh(mesh.devices.reshape(mesh.shape["ep"], 4, 4), ("ep", "tp_0", "tp_1"))
    return jax.shard_map(
        shards,
        mesh=split,
        in_specs=(
            P("ep", TP),
            P("ep", TP),
            P("ep", TP),
            P("ep", TP),
            P(EP_TP, None),
            P(),
            P("ep", None),
            P(EP_TP, None),
            P("ep", TP, None),
            P("ep", TP, None),
            P("ep", TP, None),
            P(TP, None),
            P(TP, None),
            P(TP, None),
        ),
        out_specs=(P("ep", TP), P(EP_TP, None)),
        check_vma=False,
    )
```

```python
import functools

import jax
import jax.numpy as jnp
from jax import lax
from jax.experimental import pallas as pl
from jax.experimental.pallas import tpu as pltpu
from jax.sharding import Mesh
from jax.sharding import PartitionSpec as P

TP = ("tp_0", "tp_1")
EP_TP = ("ep", "tp_0", "tp_1")


norm_eps = 1e-05
MESH = pl.DeviceIdType.MESH


def packed_rows(keys, values, key_bias):
    num_rows, width = keys.shape
    bias_rows = key_bias.reshape(num_rows // width, width)
    return jnp.concatenate(
        [keys, values, jnp.pad(bias_rows, ((0, 16 - bias_rows.shape[0]), (0, 0)))], axis=0
    )


def attention_kernel(scale_factor, q_ref, kv_ref, o_ref, tri, acc, later):
    num_rows, width = q_ref.shape
    chunk = 128
    me = lax.axis_index("ep")
    row_id = lax.broadcasted_iota(jnp.int32, (num_rows, num_rows + 128), 0)
    col_id = lax.broadcasted_iota(jnp.int32, (num_rows, num_rows + 128), 1)
    tri[...] = jnp.where((row_id > col_id) | (col_id >= num_rows), -1.0, 0.0).astype(jnp.bfloat16)
    acc[...] = jnp.zeros_like(acc)
    later[...] = jnp.zeros_like(later)

    def visit(block, diagonal):
        k_block = kv_ref[block, :num_rows, :]
        v_block = kv_ref[block, num_rows : 2 * num_rows, :]
        bias = kv_ref[block, 2 * num_rows : 2 * num_rows + 16, :].astype(jnp.float32)
        bias = jnp.concatenate([bias[r : r + 1] for r in range(num_rows // width)], axis=1)
        for first in range(0, num_rows, chunk):
            rows = slice(first, first + chunk)
            scores = (
                lax.dot_general(
                    q_ref[rows, :],
                    k_block,
                    (((1,), (1,)), ((), ())),
                    preferred_element_type=jnp.float32,
                )
                * scale_factor
                + bias
            )
            soft = jnp.maximum(scores, jnp.log(1.0 + jnp.exp(jnp.minimum(scores, 88.0))))
            dropped = soft
            if diagonal:
                causal = lax.broadcasted_iota(
                    jnp.int32, scores.shape, 1
                ) < first + lax.broadcasted_iota(jnp.int32, scores.shape, 0)
                dropped = jnp.where(causal, soft, 0.0)
            sums = jnp.dot(
                dropped.astype(jnp.bfloat16), tri[...], preferred_element_type=jnp.float32
            )
            carried = later[rows, :]
            between = sums[:, :num_rows] + jnp.concatenate(
                [carried] * (num_rows // width), axis=1
            )
            weights = jnp.exp(scores - soft + between)
            if diagonal:
                weights = jnp.where(causal, weights, 0.0)
            acc[rows, :] += jnp.dot(
                weights.astype(jnp.bfloat16), v_block, preferred_element_type=jnp.float32
            )
            later[rows, :] = carried + sums[:, num_rows:]

    visit(me, True)

    def earlier(count, carry):
        visit(me - 1 - count, False)
        return carry

    lax.fori_loop(0, me, earlier, 0)
    raw_out = acc[...]
    o_ref[...] = (
        raw_out * lax.rsqrt(jnp.mean(raw_out * raw_out, axis=1, keepdims=True) + norm_eps)
    ).astype(jnp.bfloat16)


def stick_half(queries, keys, values, key_bias):
    num_rows, width = queries.shape
    filled = lax.all_gather(packed_rows(keys, values, key_bias), "ep", axis=0, tiled=False)
    return pl.pallas_call(
        functools.partial(attention_kernel, width ** (-0.5)),
        out_shape=jax.ShapeDtypeStruct((num_rows, width), jnp.bfloat16),
        in_specs=[pl.BlockSpec(memory_space=pltpu.VMEM)] * 2,
        out_specs=pl.BlockSpec(memory_space=pltpu.VMEM),
        scratch_shapes=[
            pltpu.VMEM((num_rows, num_rows + 128), jnp.bfloat16),
            pltpu.VMEM((num_rows, width), jnp.float32),
            pltpu.VMEM((num_rows, 128), jnp.float32),
        ],
        compiler_params=pltpu.CompilerParams(vmem_limit_bytes=40 * 1024 * 1024),
        cost_estimate=pl.CostEstimate(
            flops=8_000_000_000, bytes_accessed=7_000_000, transcendentals=14_000_000
        ),
    )(queries, filled)


def expert_kernel(
    moe_in,
    gain,
    ids,
    ids_across,
    mix,
    gate,
    up,
    down,
    shared_gate,
    shared_up,
    shared_down,
    out,
    w_in,
    w_out,
    w_shared,
    cut,
    mixes,
    pre,
    outgoing,
    pooled,
    partial,
    inbox,
    result,
    shared_sum,
    returned,
    comb,
    cut_back,
    landed,
    w_sem,
    pre_send,
    pre_recv,
    mix_send,
    mix_recv,
    go_send,
    go_recv,
    ag_send,
    ag_recv,
    rs_send,
    rs_recv,
    back_send,
    back_recv,
    fin_send,
    fin_recv,
):
    ep_count, tp_count = lax.axis_size("ep"), 16
    rows = moe_in.shape[0]
    e = lax.axis_index("ep")
    y = lax.axis_index("tp_0")
    x = lax.axis_index("tp_1")
    t = y * 4 + x

    def tp_peer(k):
        other = lax.rem(t + k, tp_count)
        return other, {"tp_0": other // 4, "tp_1": lax.rem(other, 4)}

    barrier = pltpu.get_barrier_semaphore()

    def greet_tp(k, carry):
        pl.semaphore_signal(barrier, inc=1, device_id=tp_peer(k)[1], device_id_type=MESH)
        return carry

    def greet_ep(k, carry):
        pl.semaphore_signal(
            barrier, inc=1, device_id={"ep": lax.rem(e + k, ep_count)}, device_id_type=MESH
        )
        return carry

    lax.fori_loop(1, ep_count, greet_ep, 0)
    lax.fori_loop(1, tp_count, greet_tp, 0)

    loads = [
        pltpu.make_async_copy(gate, w_in.at[pl.ds(0, 2)], w_sem.at[0]),
        pltpu.make_async_copy(up, w_in.at[pl.ds(2, 2)], w_sem.at[1]),
        pltpu.make_async_copy(down, w_out, w_sem.at[2]),
        pltpu.make_async_copy(shared_gate, w_shared.at[0], w_sem.at[3]),
        pltpu.make_async_copy(shared_up, w_shared.at[1], w_sem.at[4]),
        pltpu.make_async_copy(shared_down, w_shared.at[2], w_sem.at[5]),
    ]
    for load in loads:
        load.start()

    as_float = moe_in[...].astype(jnp.float32)
    normed = (
        as_float
        * lax.rsqrt(jnp.mean(as_float * as_float, axis=1, keepdims=True) + norm_eps)
        * gain[...]
    ).astype(jnp.bfloat16)
    for k in range(tp_count):
        cut[k] = normed[:, k * 128 : (k + 1) * 128]
    own_ids = ids[pl.ds(pl.multiple_of(t * rows, rows), rows), :]
    own_mix = mix[...]
    lane = lax.broadcasted_iota(jnp.int32, (rows, 128), 1)
    spread = jnp.zeros((rows, 128), jnp.float32)
    for k in range(mix.shape[1]):
        spread = spread + jnp.where(own_ids[:, k : k + 1] == lane, own_mix[:, k : k + 1], 0.0)
    mixes[t] = spread
    pre[t] = cut[t]

    pl.semaphore_wait(barrier, ep_count + tp_count - 2)

    def send_pre(k, carry):
        other, device = tp_peer(k)
        pltpu.make_async_remote_copy(
            cut.at[other], pre.at[t], pre_send, pre_recv, device_id=device, device_id_type=MESH
        ).start()
        return carry

    def send_mix(k, carry):
        _, device = tp_peer(k)
        pltpu.make_async_remote_copy(
            mixes.at[t], mixes.at[t], mix_send, mix_recv, device_id=device, device_id_type=MESH
        ).start()
        return carry

    lax.fori_loop(1, tp_count, send_pre, 0)
    lax.fori_loop(1, tp_count, send_mix, 0)

    across = ids_across[...]
    expert_id = lax.broadcasted_iota(jnp.int32, (64, 128), 0)
    named = across[0:1] == expert_id
    for k in range(1, across.shape[0]):
        named = named | (across[k : k + 1] == expert_id)
    named = named.astype(jnp.float32)
    source = lax.broadcasted_iota(jnp.int32, (tp_count, 128), 0)
    same = (lax.broadcasted_iota(jnp.int32, (tp_count, 128), 1) // rows == source).astype(
        jnp.float32
    )
    for k in range(64):
        outgoing[k * 16 : (k + 1) * 16, :] = (same * named[k : k + 1, :]).astype(jnp.bfloat16)

    pltpu.make_async_copy(
        pre.at[pl.ds(0, tp_count - 1)], pre.at[pl.ds(0, tp_count - 1)], pre_recv
    ).wait()
    own_rows = pre[...].astype(jnp.float32).reshape(tp_count * rows, 128).astype(jnp.bfloat16)
    pooled[t, 1024:1152, :] = own_rows
    for k in range(4):
        part = slice(k * 256, (k + 1) * 256)
        outgoing[part, :] = jnp.dot(
            outgoing[part, :], own_rows, preferred_element_type=jnp.float32
        ).astype(jnp.bfloat16)
    at_e = pl.ds(pl.multiple_of(e * 32, 32), 32)

    def send_go(k, carry):
        other = lax.rem(e + k, ep_count)
        pltpu.make_async_remote_copy(
            outgoing.at[pl.ds(pl.multiple_of(other * 32, 32), 32)],
            pooled.at[t, at_e],
            go_send,
            go_recv,
            device_id={"ep": other},
            device_id_type=MESH,
        ).start()
        return carry

    lax.fori_loop(1, ep_count, send_go, 0)
    pooled[t, at_e, :] = outgoing[at_e, :]

    pltpu.make_async_copy(
        mixes.at[pl.ds(0, tp_count - 1)], mixes.at[pl.ds(0, tp_count - 1)], mix_recv
    ).wait()
    mix_all = mixes[...].reshape(tp_count * rows, 128)
    high = mix_all.astype(jnp.bfloat16)
    low = (mix_all - high.astype(jnp.float32)).astype(jnp.bfloat16)
    for k in range(4):
        column = k * 256 + lax.broadcasted_iota(jnp.int32, (128, 256), 1)
        row = lax.broadcasted_iota(jnp.int32, (128, 256), 0)
        widen = (column // 16 == row).astype(jnp.bfloat16)
        keep = lax.rem(column, 16) == row // rows
        for part, value in ((0, high), (1, low)):
            wide = jnp.dot(value, widen, preferred_element_type=jnp.float32)
            comb[part, :, k * 256 : (k + 1) * 256] = jnp.where(keep, wide, 0.0).astype(
                jnp.bfloat16
            )

    pltpu.make_async_copy(
        pooled.at[t, pl.ds(0, 992)], pooled.at[t, pl.ds(0, 992)], go_recv
    ).wait()

    quarter = 288
    names = ("tp_0", "tp_1")
    place = {"tp_0": y, "tp_1": x}

    def axes(q):
        first, second = names if q < 2 else names[::-1]
        return first, second, 1 if q % 2 == 0 else 3

    def index_at(q, df, dg):
        first, second, _ = axes(q)
        moved = {
            first: lax.rem(place[first] + df % 4, 4),
            second: lax.rem(place[second] + dg % 4, 4),
        }
        return moved["tp_0"] * 4 + moved["tp_1"]

    def block(ref, q, df, dg):
        return ref.at[index_at(q, df, dg), pl.ds(q * quarter, quarter)]

    def ag_copy(q, df, dg, along_first, step):
        first, second, _ = axes(q)
        axis = first if along_first else second
        there = ((df - step) % 4, dg % 4) if along_first else (df % 4, (dg - step) % 4)
        ref = block(pooled, q, df, dg)
        return pltpu.make_async_remote_copy(
            ref,
            ref,
            ag_send,
            ag_recv.at[q, there[0] * 4 + there[1]],
            device_id={axis: lax.rem(place[axis] + step % 4, 4)},
            device_id_type=MESH,
        )

    def ag_wait(q, df, dg):
        ref = block(pooled, q, df, dg)
        pltpu.make_async_copy(ref, ref, ag_recv.at[q, (df % 4) * 4 + dg % 4]).wait()

    quarters = range(4)
    for q in quarters:
        ag_copy(q, 0, 0, True, 1).start()
        ag_copy(q, 0, 0, True, 3).start()
    for q in quarters:
        ag_copy(q, 0, 0, False, 1).start()
        ag_copy(q, 0, 0, False, 3).start()
    for q in quarters:
        d = axes(q)[2]
        ag_wait(q, -d, 0)
        ag_copy(q, -d, 0, True, d).start()
        ag_copy(q, -d, 0, False, 1).start()
        ag_copy(q, -d, 0, False, 3).start()
    for q in quarters:
        d = axes(q)[2]
        ag_wait(q, d, 0)
        ag_copy(q, d, 0, False, 1).start()
        ag_copy(q, d, 0, False, 3).start()
    for q in quarters:
        d = axes(q)[2]
        ag_wait(q, 0, -d)
        ag_copy(q, 0, -d, False, d).start()
    for q in quarters:
        ag_wait(q, 2, 0)
        ag_copy(q, 2, 0, False, 1).start()
        ag_copy(q, 2, 0, False, 3).start()
    for hop in range(3):
        for q in quarters:
            d = axes(q)[2]
            df = (-d, d, 2)[hop]
            ag_wait(q, df, -d)
            ag_copy(q, df, -d, False, d).start()

    for load in loads:
        load.wait()

    def rs_copy(q, ref, slot, along_first, step):
        first, second, _ = axes(q)
        axis = first if along_first else second
        return pltpu.make_async_remote_copy(
            ref,
            inbox.at[q, slot],
            rs_send,
            rs_recv.at[q, slot],
            device_id={axis: lax.rem(place[axis] + step % 4, 4)},
            device_id_type=MESH,
        )

    def rs_wait(q, slot):
        ref = inbox.at[q, slot]
        pltpu.make_async_copy(ref, ref, rs_recv.at[q, slot]).wait()

    def plus(q, df, dg, *slots):
        where = index_at(q, df, dg)
        total = partial[where, q * quarter : (q + 1) * quarter, :].astype(jnp.float32)
        for slot in slots:
            total = total + inbox[q, slot].astype(jnp.float32)
        return where, total

    def silu_times(both):
        half = both.shape[1] // 2
        gate_val = both[:, :half]
        return gate_val * (1.0 / (1.0 + jnp.exp(-gate_val))) * both[:, half:]

    def feed(span, weights_in, weights_out, routed):
        both = jnp.concatenate([pooled[k, span, :] for k in range(tp_count)], axis=1)
        hidden = silu_times(
            lax.dot_general(
                both, weights_in, (((1,), (1,)), ((), ())), preferred_element_type=jnp.float32
            )
        )
        if routed:
            row = lax.broadcasted_iota(jnp.int32, hidden.shape, 0)
            column = lax.broadcasted_iota(jnp.int32, hidden.shape, 1)
            hidden = jnp.where(lax.rem(row // 16, 2) == column // 64, hidden, 0.0)
        hidden = hidden.astype(jnp.bfloat16)
        for k in range(0, tp_count, 2):
            term = jnp.dot(
                hidden,
                weights_out[:, k * 128 : (k + 2) * 128],
                preferred_element_type=jnp.float32,
            ).astype(jnp.bfloat16)
            partial[k, span, :] = term[:, :128]
            partial[k + 1, span, :] = term[:, 128:]

    for q in quarters:
        d = axes(q)[2]
        for df in range(4):
            ag_wait(q, df, d)
            ag_wait(q, df, 2)
        last = q == 3
        span = slice(q * quarter, 1024 if last else (q + 1) * quarter)
        feed(span, w_in[...].reshape(256, 2048), w_out[...].reshape(128, 2048), True)
        if last:
            feed(
                slice(1024, 1152), w_shared[0:2].reshape(128, 2048), w_shared[2], False
            )
        for df in (2, -d, d, 0):
            slot = (df % 4) * 3
            rs_copy(q, block(partial, q, df, 2), slot, False, d).start()
            rs_copy(q, block(partial, q, df, -d), slot + 1, False, -d).start()

    rows_of = lambda q: slice(q * quarter, (q + 1) * quarter)
    for turn in range(4):
        for q in quarters:
            d = axes(q)[2]
            df = (2, -d, d, 0)[turn] % 4
            rs_wait(q, df * 3)
            where, total = plus(q, df, d, df * 3)
            partial[where, rows_of(q), :] = total.astype(jnp.bfloat16)
            rs_copy(q, block(partial, q, df, d), df * 3 + 2, False, d).start()
    for turn in range(4):
        for q in quarters:
            d = axes(q)[2]
            df = (2, -d, d, 0)[turn] % 4
            rs_wait(q, df * 3 + 1)
            rs_wait(q, df * 3 + 2)
            slots = [df * 3 + 1, df * 3 + 2]
            if turn == 2:
                rs_wait(q, 12)
                slots.append(12)
            where, total = plus(q, df, 0, *slots)
            partial[where, rows_of(q), :] = total.astype(jnp.bfloat16)
            if turn == 0:
                rs_copy(q, block(partial, q, df, 0), 12, True, d).start()
            elif turn == 1:
                rs_copy(q, block(partial, q, df, 0), 13, True, -d).start()
            elif turn == 2:
                rs_copy(q, block(partial, q, df, 0), 14, True, d).start()

    for q in quarters:
        rs_wait(q, 13)
        rs_wait(q, 14)
        _, total = plus(q, 0, 0, 13, 14)
        result[rows_of(q), :] = total.astype(jnp.bfloat16)
        if q == 3:
            shared_sum[...] = total[160:288, :]

        def send_back(other, carry):
            @pl.when(other != e)
            def _():
                pltpu.make_async_remote_copy(
                    result.at[pl.ds(pl.multiple_of(other * 32, 32), 32)],
                    returned.at[at_e],
                    back_send,
                    back_recv,
                    device_id={"ep": other},
                    device_id_type=MESH,
                ).start()

            return carry

        lax.fori_loop(q * 9, min(ep_count, (q + 1) * 9), send_back, 0)
    returned[at_e, :] = result[at_e, :]
    pltpu.make_async_copy(
        returned.at[pl.ds(0, 992)], returned.at[pl.ds(0, 992)], back_recv
    ).wait()
    combined = (
        shared_sum[...]
        + jnp.dot(comb[0], returned[...], preferred_element_type=jnp.float32)
        + jnp.dot(comb[1], returned[...], preferred_element_type=jnp.float32)
    )
    for k in range(tp_count):
        cut_back[k] = combined[k * rows : (k + 1) * rows, :].astype(jnp.bfloat16)

    def send_fin(k, carry):
        other, device = tp_peer(k)
        pltpu.make_async_remote_copy(
            cut_back.at[other],
            landed.at[t],
            fin_send,
            fin_recv,
            device_id=device,
            device_id_type=MESH,
        ).start()
        return carry

    lax.fori_loop(1, tp_count, send_fin, 0)
    landed[t] = cut_back[t]

    most = tp_count - 1
    for ref, sem in (
        (pre.at[pl.ds(0, most)], pre_send),
        (mixes.at[pl.ds(0, most)], mix_send),
        (outgoing.at[pl.ds(0, 992)], go_send),
        (pooled.at[pl.ds(0, most)], ag_send),
        (partial.at[pl.ds(0, most)], rs_send),
        (result.at[pl.ds(0, 992)], back_send),
        (landed.at[pl.ds(0, most)], fin_recv),
        (landed.at[pl.ds(0, most)], fin_send),
    ):
        pltpu.make_async_copy(ref, ref, sem).wait()
    for k in range(tp_count):
        out[:, k * 128 : (k + 1) * 128] = landed[k]


def expert_half(
    moe_in,
    norm_gain,
    route_ids,
    route_weights,
    gate_weight,
    up_weight,
    down_weight,
    shared_gate,
    shared_up,
    shared_down,
):
    own_rows, width = moe_in.shape
    hidden = gate_weight.shape[1]
    bf16, f32 = jnp.bfloat16, jnp.float32
    vmem, dma = pltpu.VMEM, pltpu.SemaphoreType.DMA
    here, there = pl.BlockSpec(memory_space=pltpu.VMEM), pl.BlockSpec(memory_space=pl.ANY)
    return pl.pallas_call(
        expert_kernel,
        out_shape=jax.ShapeDtypeStruct((own_rows, width), bf16),
        in_specs=[here] * 5 + [there] * 6,
        out_specs=here,
        scratch_shapes=[
            vmem((4, hidden, width), bf16),
            vmem((2, hidden, width), bf16),
            vmem((3, hidden, width), bf16),
            vmem((16, own_rows, 128), bf16),
            vmem((16, own_rows, 128), f32),
            vmem((16, own_rows, 128), bf16),
            vmem((1024, 128), bf16),
            vmem((16, 1152, 128), bf16),
            vmem((16, 1152, 128), bf16),
            vmem((4, 15, 288, 128), bf16),
            vmem((1152, 128), bf16),
            vmem((128, 128), f32),
            vmem((1024, 128), bf16),
            vmem((2, 128, 1024), bf16),
            vmem((16, own_rows, 128), bf16),
            vmem((16, own_rows, 128), bf16),
            dma((6,)),
            dma,
            dma,
            dma,
            dma,
            dma,
            dma,
            dma,
            dma((4, 16)),
            dma,
            dma((4, 15)),
            dma,
            dma,
            dma,
            dma,
        ],
        compiler_params=pltpu.CompilerParams(
            collective_id=0, has_side_effects=True, vmem_limit_bytes=40 * 1024 * 1024
        ),
        cost_estimate=pl.CostEstimate(
            flops=80_000_000_000, bytes_accessed=200_000_000, transcendentals=300_000
        ),
    )(
        moe_in,
        norm_gain[None, :],
        route_ids,
        route_ids.T,
        route_weights,
        gate_weight,
        up_weight,
        down_weight,
        shared_gate,
        shared_up,
        shared_down,
    )


def shards(
    queries,
    keys,
    values,
    key_bias,
    moe_in,
    norm_gain,
    route_ids,
    route_weights,
    gate_weight,
    up_weight,
    down_weight,
    shared_gate,
    shared_up,
    shared_down,
):
    heads_out = stick_half(queries, keys, values, key_bias)
    moe_out = expert_half(
        moe_in,
        norm_gain,
        route_ids,
        route_weights,
        gate_weight,
        up_weight,
        down_weight,
        shared_gate,
        shared_up,
        shared_down,
    )
    return (heads_out, moe_out)


def solution(mesh):
    split = Mesh(mesh.devices.reshape(mesh.shape["ep"], 4, 4), ("ep", "tp_0", "tp_1"))
    return jax.shard_map(
        shards,
        mesh=split,
        in_specs=(
            P("ep", TP),
            P("ep", TP),
            P("ep", TP),
            P("ep", TP),
            P(EP_TP, None),
            P(),
            P("ep", None),
            P(EP_TP, None),
            P("ep", TP, None),
            P("ep", TP, None),
            P("ep", TP, None),
            P(TP, None),
            P(TP, None),
            P(TP, None),
        ),
        out_specs=(P("ep", TP), P(EP_TP, None)),
        check_vma=False,
    )
```

```python
import functools

import jax
import jax.numpy as jnp
from jax import lax
from jax.experimental import pallas as pl
from jax.experimental.pallas import tpu as pltpu
from jax.sharding import Mesh
from jax.sharding import PartitionSpec as P

TP = ("tp_0", "tp_1")
EP_TP = ("ep", "tp_0", "tp_1")


norm_eps = 1e-05
MESH = pl.DeviceIdType.MESH


def packed_rows(keys, values, key_bias):
    num_rows, width = keys.shape
    bias_rows = key_bias.reshape(num_rows // width, width)
    return jnp.concatenate(
        [keys, values, jnp.pad(bias_rows, ((0, 16 - bias_rows.shape[0]), (0, 0)))], axis=0
    )


FAR = -1e30


def attention_start(state, row_count):
    scores_ref, logit_ref, sums_ref, soft_ref, weight_ref, tri, acc, later = state
    row_id = lax.broadcasted_iota(jnp.int32, tri.shape, 0)
    col_id = lax.broadcasted_iota(jnp.int32, tri.shape, 1)
    tri[...] = jnp.where((row_id > col_id) | (col_id >= 128), -1.0, 0.0).astype(jnp.bfloat16)
    acc[...] = jnp.zeros_like(acc)
    later[...] = jnp.zeros_like(later)
    sums_ref[...] = jnp.zeros_like(sums_ref)
    logit_ref[...] = jnp.full(logit_ref.shape, FAR, jnp.float32)
    scores_ref[...] = jnp.full(scores_ref.shape, FAR, jnp.float32)


def attention_finish_block(state, v_block):
    scores_ref, logit_ref, sums_ref, soft_ref, weight_ref, tri, acc, later = state
    num_rows = scores_ref.shape[0]
    piece = 16
    for first in range(0, num_rows, piece):
        carried = later[first : first + piece, :]
        for c in reversed(range(num_rows // 128)):
            at = c * num_rows + first
            weight_ref[first : first + piece, c * 128 : (c + 1) * 128] = jnp.exp(
                logit_ref[first : first + piece, c * 128 : (c + 1) * 128]
                + (sums_ref[at : at + piece, :128] + carried)
            ).astype(jnp.bfloat16)
            carried = carried + sums_ref[at : at + piece, 128:]
        later[first : first + piece, :] = carried
    acc[...] += jnp.dot(weight_ref[...], v_block, preferred_element_type=jnp.float32)


def attention_sum_block(state):
    scores_ref, logit_ref, sums_ref, soft_ref, weight_ref, tri, acc, later = state
    num_rows = scores_ref.shape[0]
    piece = 16
    for c in range(num_rows // 128):
        columns = slice(c * 128, (c + 1) * 128)
        for first in range(0, num_rows, piece):
            scores = scores_ref[first : first + piece, columns]
            soft = jnp.maximum(scores, jnp.log(1.0 + jnp.exp(jnp.minimum(scores, 88.0))))
            logit_ref[first : first + piece, columns] = scores - soft
            soft_ref[c * num_rows + first : c * num_rows + first + piece, :] = soft.astype(
                jnp.bfloat16
            )
    sums_ref[...] = jnp.dot(soft_ref[...], tri[...], preferred_element_type=jnp.float32)


def attention_score_block(state, q_ref, k_block, bias_rows, diagonal):
    scores_ref = state[0]
    num_rows, width = q_ref.shape
    bias = bias_rows.astype(jnp.float32)
    bias = jnp.concatenate([bias[r : r + 1] for r in range(num_rows // width)], axis=1)
    products = lax.dot_general(
        q_ref[...], k_block, (((1,), (1,)), ((), ())), preferred_element_type=jnp.float32
    )
    scores = products * width ** (-0.5) + bias
    if diagonal:
        causal = lax.broadcasted_iota(jnp.int32, scores.shape, 1) < lax.broadcasted_iota(
            jnp.int32, scores.shape, 0
        )
        scores = jnp.where(causal, scores, FAR)
    scores_ref[...] = scores


def attention_parts(kv_ref, block, num_rows):
    return (
        kv_ref[block, :num_rows, :],
        kv_ref[block, num_rows : 2 * num_rows, :],
        kv_ref[block, 2 * num_rows : 2 * num_rows + 16, :],
    )


def attention_step(state, q_ref, kv_ref, me, count):
    num_rows = q_ref.shape[0]
    v_block = attention_parts(kv_ref, jnp.minimum(me - count + 2, me), num_rows)[1]
    k_block, _, bias_rows = attention_parts(kv_ref, jnp.maximum(me - count, 0), num_rows)
    attention_finish_block(state, v_block)
    attention_sum_block(state)
    attention_score_block(state, q_ref, k_block, bias_rows, False)


def attention_end(state, o_ref):
    raw_out = state[6][...]
    o_ref[...] = (
        raw_out * lax.rsqrt(jnp.mean(raw_out * raw_out, axis=1, keepdims=True) + norm_eps)
    ).astype(jnp.bfloat16)


def attention_kernel(q_ref, kv_ref, o_ref, *state):
    num_rows = q_ref.shape[0]
    me = lax.axis_index("ep")
    attention_start(state, num_rows)
    k_block, _, bias_rows = attention_parts(kv_ref, me, num_rows)
    attention_score_block(state, q_ref, k_block, bias_rows, True)

    def step(count, carry):
        attention_step(state, q_ref, kv_ref, me, count)
        return carry

    lax.fori_loop(1, me + 3, step, 0)
    attention_end(state, o_ref)


def attention_state(num_rows, width):
    f32, bf16 = jnp.float32, jnp.bfloat16
    pieces = num_rows // 128
    return [
        pltpu.VMEM((num_rows, num_rows), f32),
        pltpu.VMEM((num_rows, num_rows), f32),
        pltpu.VMEM((pieces * num_rows, 256), f32),
        pltpu.VMEM((pieces * num_rows, 128), bf16),
        pltpu.VMEM((num_rows, num_rows), bf16),
        pltpu.VMEM((128, 256), bf16),
        pltpu.VMEM((num_rows, width), f32),
        pltpu.VMEM((num_rows, 128), f32),
    ]


def stick_half(queries, keys, values, key_bias):
    num_rows, width = queries.shape
    filled = lax.all_gather(packed_rows(keys, values, key_bias), "ep", axis=0, tiled=False)
    return pl.pallas_call(
        attention_kernel,
        out_shape=jax.ShapeDtypeStruct((num_rows, width), jnp.bfloat16),
        in_specs=[pl.BlockSpec(memory_space=pltpu.VMEM)] * 2,
        out_specs=pl.BlockSpec(memory_space=pltpu.VMEM),
        scratch_shapes=attention_state(num_rows, width),
        compiler_params=pltpu.CompilerParams(vmem_limit_bytes=60 * 1024 * 1024),
        cost_estimate=pl.CostEstimate(
            flops=8_000_000_000, bytes_accessed=7_000_000, transcendentals=14_000_000
        ),
    )(queries, filled)


def expert_kernel(
    moe_in,
    gain,
    ids,
    ids_across,
    mix,
    gate,
    up,
    down,
    shared_gate,
    shared_up,
    shared_down,
    out,
    w_in,
    w_out,
    w_shared,
    cut,
    mixes,
    pre,
    outgoing,
    pooled,
    partial,
    inbox,
    result,
    shared_sum,
    returned,
    comb,
    cut_back,
    landed,
    w_sem,
    pre_send,
    pre_recv,
    mix_send,
    mix_recv,
    go_send,
    go_recv,
    ag_send,
    ag_recv,
    rs_send,
    rs_recv,
    back_send,
    back_recv,
    fin_send,
    fin_recv,
):
    ep_count, tp_count = lax.axis_size("ep"), 16
    rows = moe_in.shape[0]
    e = lax.axis_index("ep")
    y = lax.axis_index("tp_0")
    x = lax.axis_index("tp_1")
    t = y * 4 + x

    def tp_peer(k):
        other = lax.rem(t + k, tp_count)
        return other, {"tp_0": other // 4, "tp_1": lax.rem(other, 4)}

    barrier = pltpu.get_barrier_semaphore()

    def greet_tp(k, carry):
        pl.semaphore_signal(barrier, inc=1, device_id=tp_peer(k)[1], device_id_type=MESH)
        return carry

    def greet_ep(k, carry):
        pl.semaphore_signal(
            barrier, inc=1, device_id={"ep": lax.rem(e + k, ep_count)}, device_id_type=MESH
        )
        return carry

    lax.fori_loop(1, ep_count, greet_ep, 0)
    lax.fori_loop(1, tp_count, greet_tp, 0)

    loads = [
        pltpu.make_async_copy(gate, w_in.at[pl.ds(0, 2)], w_sem.at[0]),
        pltpu.make_async_copy(up, w_in.at[pl.ds(2, 2)], w_sem.at[1]),
        pltpu.make_async_copy(down, w_out, w_sem.at[2]),
        pltpu.make_async_copy(shared_gate, w_shared.at[0], w_sem.at[3]),
        pltpu.make_async_copy(shared_up, w_shared.at[1], w_sem.at[4]),
        pltpu.make_async_copy(shared_down, w_shared.at[2], w_sem.at[5]),
    ]
    for load in loads:
        load.start()

    as_float = moe_in[...].astype(jnp.float32)
    normed = (
        as_float
        * lax.rsqrt(jnp.mean(as_float * as_float, axis=1, keepdims=True) + norm_eps)
        * gain[...]
    ).astype(jnp.bfloat16)
    for k in range(tp_count):
        cut[k] = normed[:, k * 128 : (k + 1) * 128]
    own_ids = ids[pl.ds(pl.multiple_of(t * rows, rows), rows), :]
    own_mix = mix[...]
    lane = lax.broadcasted_iota(jnp.int32, (rows, 128), 1)
    spread = jnp.zeros((rows, 128), jnp.float32)
    for k in range(mix.shape[1]):
        spread = spread + jnp.where(own_ids[:, k : k + 1] == lane, own_mix[:, k : k + 1], 0.0)
    mixes[t] = spread
    pre[t] = cut[t]

    pl.semaphore_wait(barrier, ep_count + tp_count - 2)

    def send_pre(k, carry):
        other, device = tp_peer(k)
        pltpu.make_async_remote_copy(
            cut.at[other], pre.at[t], pre_send, pre_recv, device_id=device, device_id_type=MESH
        ).start()
        return carry

    def send_mix(k, carry):
        _, device = tp_peer(k)
        pltpu.make_async_remote_copy(
            mixes.at[t], mixes.at[t], mix_send, mix_recv, device_id=device, device_id_type=MESH
        ).start()
        return carry

    lax.fori_loop(1, tp_count, send_pre, 0)
    lax.fori_loop(1, tp_count, send_mix, 0)

    across = ids_across[...]
    expert_id = lax.broadcasted_iota(jnp.int32, (64, 128), 0)
    named = across[0:1] == expert_id
    for k in range(1, across.shape[0]):
        named = named | (across[k : k + 1] == expert_id)
    named = named.astype(jnp.float32)
    source = lax.broadcasted_iota(jnp.int32, (tp_count, 128), 0)
    same = (lax.broadcasted_iota(jnp.int32, (tp_count, 128), 1) // rows == source).astype(
        jnp.float32
    )
    for k in range(64):
        outgoing[k * 16 : (k + 1) * 16, :] = (same * named[k : k + 1, :]).astype(jnp.bfloat16)

    pltpu.make_async_copy(
        pre.at[pl.ds(0, tp_count - 1)], pre.at[pl.ds(0, tp_count - 1)], pre_recv
    ).wait()
    own_rows = pre[...].astype(jnp.float32).reshape(tp_count * rows, 128).astype(jnp.bfloat16)
    pooled[t, 1024:1152, :] = own_rows
    for k in range(4):
        part = slice(k * 256, (k + 1) * 256)
        outgoing[part, :] = jnp.dot(
            outgoing[part, :], own_rows, preferred_element_type=jnp.float32
        ).astype(jnp.bfloat16)
    at_e = pl.ds(pl.multiple_of(e * 32, 32), 32)

    def send_go(k, carry):
        other = lax.rem(e + k, ep_count)
        pltpu.make_async_remote_copy(
            outgoing.at[pl.ds(pl.multiple_of(other * 32, 32), 32)],
            pooled.at[t, at_e],
            go_send,
            go_recv,
            device_id={"ep": other},
            device_id_type=MESH,
        ).start()
        return carry

    lax.fori_loop(1, ep_count, send_go, 0)
    pooled[t, at_e, :] = outgoing[at_e, :]

    pltpu.make_async_copy(
        mixes.at[pl.ds(0, tp_count - 1)], mixes.at[pl.ds(0, tp_count - 1)], mix_recv
    ).wait()
    mix_all = mixes[...].reshape(tp_count * rows, 128)
    high = mix_all.astype(jnp.bfloat16)
    low = (mix_all - high.astype(jnp.float32)).astype(jnp.bfloat16)
    for k in range(4):
        column = k * 256 + lax.broadcasted_iota(jnp.int32, (128, 256), 1)
        row = lax.broadcasted_iota(jnp.int32, (128, 256), 0)
        widen = (column // 16 == row).astype(jnp.bfloat16)
        keep = lax.rem(column, 16) == row // rows
        for part, value in ((0, high), (1, low)):
            wide = jnp.dot(value, widen, preferred_element_type=jnp.float32)
            comb[part, :, k * 256 : (k + 1) * 256] = jnp.where(keep, wide, 0.0).astype(
                jnp.bfloat16
            )

    pltpu.make_async_copy(
        pooled.at[t, pl.ds(0, 992)], pooled.at[t, pl.ds(0, 992)], go_recv
    ).wait()

    quarter = 288
    names = ("tp_0", "tp_1")
    place = {"tp_0": y, "tp_1": x}

    def axes(q):
        first, second = names if q < 2 else names[::-1]
        return first, second, 1 if q % 2 == 0 else 3

    def index_at(q, df, dg):
        first, second, _ = axes(q)
        moved = {
            first: lax.rem(place[first] + df % 4, 4),
            second: lax.rem(place[second] + dg % 4, 4),
        }
        return moved["tp_0"] * 4 + moved["tp_1"]

    def block(ref, q, df, dg):
        return ref.at[index_at(q, df, dg), pl.ds(q * quarter, quarter)]

    def ag_copy(q, df, dg, along_first, step):
        first, second, _ = axes(q)
        axis = first if along_first else second
        there = ((df - step) % 4, dg % 4) if along_first else (df % 4, (dg - step) % 4)
        ref = block(pooled, q, df, dg)
        return pltpu.make_async_remote_copy(
            ref,
            ref,
            ag_send,
            ag_recv.at[q, there[0] * 4 + there[1]],
            device_id={axis: lax.rem(place[axis] + step % 4, 4)},
            device_id_type=MESH,
        )

    def ag_wait(q, df, dg):
        ref = block(pooled, q, df, dg)
        pltpu.make_async_copy(ref, ref, ag_recv.at[q, (df % 4) * 4 + dg % 4]).wait()

    quarters = range(4)
    for q in quarters:
        ag_copy(q, 0, 0, True, 1).start()
        ag_copy(q, 0, 0, True, 3).start()
    for q in quarters:
        ag_copy(q, 0, 0, False, 1).start()
        ag_copy(q, 0, 0, False, 3).start()
    for q in quarters:
        d = axes(q)[2]
        ag_wait(q, -d, 0)
        ag_copy(q, -d, 0, True, d).start()
        ag_copy(q, -d, 0, False, 1).start()
        ag_copy(q, -d, 0, False, 3).start()
    for q in quarters:
        d = axes(q)[2]
        ag_wait(q, d, 0)
        ag_copy(q, d, 0, False, 1).start()
        ag_copy(q, d, 0, False, 3).start()
    for q in quarters:
        d = axes(q)[2]
        ag_wait(q, 0, -d)
        ag_copy(q, 0, -d, False, d).start()
    for q in quarters:
        ag_wait(q, 2, 0)
        ag_copy(q, 2, 0, False, 1).start()
        ag_copy(q, 2, 0, False, 3).start()
    for hop in range(3):
        for q in quarters:
            d = axes(q)[2]
            df = (-d, d, 2)[hop]
            ag_wait(q, df, -d)
            ag_copy(q, df, -d, False, d).start()

    for load in loads:
        load.wait()

    def rs_copy(q, ref, slot, along_first, step):
        first, second, _ = axes(q)
        axis = first if along_first else second
        return pltpu.make_async_remote_copy(
            ref,
            inbox.at[q, slot],
            rs_send,
            rs_recv.at[q, slot],
            device_id={axis: lax.rem(place[axis] + step % 4, 4)},
            device_id_type=MESH,
        )

    def rs_wait(q, slot):
        ref = inbox.at[q, slot]
        pltpu.make_async_copy(ref, ref, rs_recv.at[q, slot]).wait()

    def plus(q, df, dg, *slots):
        where = index_at(q, df, dg)
        total = partial[where, q * quarter : (q + 1) * quarter, :].astype(jnp.float32)
        for slot in slots:
            total = total + inbox[q, slot].astype(jnp.float32)
        return where, total

    def silu_times(both):
        half = both.shape[1] // 2
        gate_val = both[:, :half]
        return gate_val * (1.0 / (1.0 + jnp.exp(-gate_val))) * both[:, half:]

    def feed(span, weights_in, weights_out, routed):
        both = jnp.concatenate([pooled[k, span, :] for k in range(tp_count)], axis=1)
        hidden = silu_times(
            lax.dot_general(
                both, weights_in, (((1,), (1,)), ((), ())), preferred_element_type=jnp.float32
            )
        )
        if routed:
            row = lax.broadcasted_iota(jnp.int32, hidden.shape, 0)
            column = lax.broadcasted_iota(jnp.int32, hidden.shape, 1)
            hidden = jnp.where(lax.rem(row // 16, 2) == column // 64, hidden, 0.0)
        hidden = hidden.astype(jnp.bfloat16)
        for k in range(0, tp_count, 2):
            term = jnp.dot(
                hidden,
                weights_out[:, k * 128 : (k + 2) * 128],
                preferred_element_type=jnp.float32,
            ).astype(jnp.bfloat16)
            partial[k, span, :] = term[:, :128]
            partial[k + 1, span, :] = term[:, 128:]

    for q in quarters:
        d = axes(q)[2]
        for df in range(4):
            ag_wait(q, df, d)
            ag_wait(q, df, 2)
        last = q == 3
        span = slice(q * quarter, 1024 if last else (q + 1) * quarter)
        feed(span, w_in[...].reshape(256, 2048), w_out[...].reshape(128, 2048), True)
        if last:
            feed(
                slice(1024, 1152), w_shared[0:2].reshape(128, 2048), w_shared[2], False
            )
        for df in (2, -d, d, 0):
            slot = (df % 4) * 3
            rs_copy(q, block(partial, q, df, 2), slot, False, d).start()
            rs_copy(q, block(partial, q, df, -d), slot + 1, False, -d).start()

    rows_of = lambda q: slice(q * quarter, (q + 1) * quarter)
    for turn in range(4):
        for q in quarters:
            d = axes(q)[2]
            df = (2, -d, d, 0)[turn] % 4
            rs_wait(q, df * 3)
            where, total = plus(q, df, d, df * 3)
            partial[where, rows_of(q), :] = total.astype(jnp.bfloat16)
            rs_copy(q, block(partial, q, df, d), df * 3 + 2, False, d).start()
    for turn in range(4):
        for q in quarters:
            d = axes(q)[2]
            df = (2, -d, d, 0)[turn] % 4
            rs_wait(q, df * 3 + 1)
            rs_wait(q, df * 3 + 2)
            slots = [df * 3 + 1, df * 3 + 2]
            if turn == 2:
                rs_wait(q, 12)
                slots.append(12)
            where, total = plus(q, df, 0, *slots)
            partial[where, rows_of(q), :] = total.astype(jnp.bfloat16)
            if turn == 0:
                rs_copy(q, block(partial, q, df, 0), 12, True, d).start()
            elif turn == 1:
                rs_copy(q, block(partial, q, df, 0), 13, True, -d).start()
            elif turn == 2:
                rs_copy(q, block(partial, q, df, 0), 14, True, d).start()

    for q in quarters:
        rs_wait(q, 13)
        rs_wait(q, 14)
        _, total = plus(q, 0, 0, 13, 14)
        result[rows_of(q), :] = total.astype(jnp.bfloat16)
        if q == 3:
            shared_sum[...] = total[160:288, :]

        def send_back(other, carry):
            @pl.when(other != e)
            def _():
                pltpu.make_async_remote_copy(
                    result.at[pl.ds(pl.multiple_of(other * 32, 32), 32)],
                    returned.at[at_e],
                    back_send,
                    back_recv,
                    device_id={"ep": other},
                    device_id_type=MESH,
                ).start()

            return carry

        lax.fori_loop(q * 9, min(ep_count, (q + 1) * 9), send_back, 0)
    returned[at_e, :] = result[at_e, :]
    pltpu.make_async_copy(
        returned.at[pl.ds(0, 992)], returned.at[pl.ds(0, 992)], back_recv
    ).wait()
    combined = (
        shared_sum[...]
        + jnp.dot(comb[0], returned[...], preferred_element_type=jnp.float32)
        + jnp.dot(comb[1], returned[...], preferred_element_type=jnp.float32)
    )
    for k in range(tp_count):
        cut_back[k] = combined[k * rows : (k + 1) * rows, :].astype(jnp.bfloat16)

    def send_fin(k, carry):
        other, device = tp_peer(k)
        pltpu.make_async_remote_copy(
            cut_back.at[other],
            landed.at[t],
            fin_send,
            fin_recv,
            device_id=device,
            device_id_type=MESH,
        ).start()
        return carry

    lax.fori_loop(1, tp_count, send_fin, 0)
    landed[t] = cut_back[t]

    most = tp_count - 1
    for ref, sem in (
        (pre.at[pl.ds(0, most)], pre_send),
        (mixes.at[pl.ds(0, most)], mix_send),
        (outgoing.at[pl.ds(0, 992)], go_send),
        (pooled.at[pl.ds(0, most)], ag_send),
        (partial.at[pl.ds(0, most)], rs_send),
        (result.at[pl.ds(0, 992)], back_send),
        (landed.at[pl.ds(0, most)], fin_recv),
        (landed.at[pl.ds(0, most)], fin_send),
    ):
        pltpu.make_async_copy(ref, ref, sem).wait()
    for k in range(tp_count):
        out[:, k * 128 : (k + 1) * 128] = landed[k]


def expert_half(
    moe_in,
    norm_gain,
    route_ids,
    route_weights,
    gate_weight,
    up_weight,
    down_weight,
    shared_gate,
    shared_up,
    shared_down,
):
    own_rows, width = moe_in.shape
    hidden = gate_weight.shape[1]
    bf16, f32 = jnp.bfloat16, jnp.float32
    vmem, dma = pltpu.VMEM, pltpu.SemaphoreType.DMA
    here, there = pl.BlockSpec(memory_space=pltpu.VMEM), pl.BlockSpec(memory_space=pl.ANY)
    return pl.pallas_call(
        expert_kernel,
        out_shape=jax.ShapeDtypeStruct((own_rows, width), bf16),
        in_specs=[here] * 5 + [there] * 6,
        out_specs=here,
        scratch_shapes=[
            vmem((4, hidden, width), bf16),
            vmem((2, hidden, width), bf16),
            vmem((3, hidden, width), bf16),
            vmem((16, own_rows, 128), bf16),
            vmem((16, own_rows, 128), f32),
            vmem((16, own_rows, 128), bf16),
            vmem((1024, 128), bf16),
            vmem((16, 1152, 128), bf16),
            vmem((16, 1152, 128), bf16),
            vmem((4, 15, 288, 128), bf16),
            vmem((1152, 128), bf16),
            vmem((128, 128), f32),
            vmem((1024, 128), bf16),
            vmem((2, 128, 1024), bf16),
            vmem((16, own_rows, 128), bf16),
            vmem((16, own_rows, 128), bf16),
            dma((6,)),
            dma,
            dma,
            dma,
            dma,
            dma,
            dma,
            dma,
            dma((4, 16)),
            dma,
            dma((4, 15)),
            dma,
            dma,
            dma,
            dma,
        ],
        compiler_params=pltpu.CompilerParams(
            collective_id=0, has_side_effects=True, vmem_limit_bytes=60 * 1024 * 1024
        ),
        cost_estimate=pl.CostEstimate(
            flops=80_000_000_000, bytes_accessed=200_000_000, transcendentals=300_000
        ),
    )(
        moe_in,
        norm_gain[None, :],
        route_ids,
        route_ids.T,
        route_weights,
        gate_weight,
        up_weight,
        down_weight,
        shared_gate,
        shared_up,
        shared_down,
    )


def shards(
    queries,
    keys,
    values,
    key_bias,
    moe_in,
    norm_gain,
    route_ids,
    route_weights,
    gate_weight,
    up_weight,
    down_weight,
    shared_gate,
    shared_up,
    shared_down,
):
    heads_out = stick_half(queries, keys, values, key_bias)
    moe_out = expert_half(
        moe_in,
        norm_gain,
        route_ids,
        route_weights,
        gate_weight,
        up_weight,
        down_weight,
        shared_gate,
        shared_up,
        shared_down,
    )
    return (heads_out, moe_out)


def solution(mesh):
    split = Mesh(mesh.devices.reshape(mesh.shape["ep"], 4, 4), ("ep", "tp_0", "tp_1"))
    return jax.shard_map(
        shards,
        mesh=split,
        in_specs=(
            P("ep", TP),
            P("ep", TP),
            P("ep", TP),
            P("ep", TP),
            P(EP_TP, None),
            P(),
            P("ep", None),
            P(EP_TP, None),
            P("ep", TP, None),
            P("ep", TP, None),
            P("ep", TP, None),
            P(TP, None),
            P(TP, None),
            P(TP, None),
        ),
        out_specs=(P("ep", TP), P(EP_TP, None)),
        check_vma=False,
    )
```

```python
import functools

import jax
import jax.numpy as jnp
from jax import lax
from jax.experimental import pallas as pl
from jax.experimental.pallas import tpu as pltpu
from jax.sharding import Mesh
from jax.sharding import PartitionSpec as P

TP = ("tp_0", "tp_1")
EP_TP = ("ep", "tp_0", "tp_1")


norm_eps = 1e-05
MESH = pl.DeviceIdType.MESH


FAR = -1e30


def attention_start(state, row_count):
    scores_ref, logit_ref, sums_ref, soft_ref, weight_ref, tri, acc, later = state
    row_id = lax.broadcasted_iota(jnp.int32, tri.shape, 0)
    col_id = lax.broadcasted_iota(jnp.int32, tri.shape, 1)
    tri[...] = jnp.where((row_id > col_id) | (col_id >= 128), -1.0, 0.0).astype(jnp.bfloat16)
    acc[...] = jnp.zeros_like(acc)
    later[...] = jnp.zeros_like(later)
    sums_ref[...] = jnp.zeros_like(sums_ref)
    logit_ref[...] = jnp.full(logit_ref.shape, FAR, jnp.float32)
    scores_ref[...] = jnp.full(scores_ref.shape, FAR, jnp.float32)


def attention_finish_block(state, v_block):
    scores_ref, logit_ref, sums_ref, soft_ref, weight_ref, tri, acc, later = state
    num_rows = scores_ref.shape[0]
    piece = 16
    for first in range(0, num_rows, piece):
        carried = later[first : first + piece, :]
        for c in reversed(range(num_rows // 128)):
            at = c * num_rows + first
            weight_ref[first : first + piece, c * 128 : (c + 1) * 128] = jnp.exp(
                logit_ref[first : first + piece, c * 128 : (c + 1) * 128]
                + (sums_ref[at : at + piece, :128] + carried)
            ).astype(jnp.bfloat16)
            carried = carried + sums_ref[at : at + piece, 128:]
        later[first : first + piece, :] = carried
    acc[...] += jnp.dot(weight_ref[...], v_block, preferred_element_type=jnp.float32)


def attention_sum_block(state):
    scores_ref, logit_ref, sums_ref, soft_ref, weight_ref, tri, acc, later = state
    num_rows = scores_ref.shape[0]
    piece = 16
    for c in range(num_rows // 128):
        columns = slice(c * 128, (c + 1) * 128)
        for first in range(0, num_rows, piece):
            scores = scores_ref[first : first + piece, columns]
            soft = jnp.maximum(scores, jnp.log(1.0 + jnp.exp(jnp.minimum(scores, 88.0))))
            logit_ref[first : first + piece, columns] = scores - soft
            soft_ref[c * num_rows + first : c * num_rows + first + piece, :] = soft.astype(
                jnp.bfloat16
            )
    sums_ref[...] = jnp.dot(soft_ref[...], tri[...], preferred_element_type=jnp.float32)


def attention_score_block(state, q_ref, k_block, bias_rows, diagonal):
    scores_ref = state[0]
    num_rows, width = q_ref.shape
    bias = bias_rows.astype(jnp.float32)
    bias = jnp.concatenate([bias[r : r + 1] for r in range(num_rows // width)], axis=1)
    products = lax.dot_general(
        q_ref[...], k_block, (((1,), (1,)), ((), ())), preferred_element_type=jnp.float32
    )
    scores = products * width ** (-0.5) + bias
    if diagonal:
        causal = lax.broadcasted_iota(jnp.int32, scores.shape, 1) < lax.broadcasted_iota(
            jnp.int32, scores.shape, 0
        )
        scores = jnp.where(causal, scores, FAR)
    scores_ref[...] = scores


def attention_parts(kv_ref, block, num_rows):
    return (
        kv_ref[block, :num_rows, :],
        kv_ref[block, num_rows : 2 * num_rows, :],
        kv_ref[block, 2 * num_rows : 2 * num_rows + 16, :],
    )


def attention_step(state, q_ref, kv_ref, me, count):
    num_rows = q_ref.shape[0]
    v_block = attention_parts(kv_ref, jnp.minimum(me - count + 2, me), num_rows)[1]
    k_block, _, bias_rows = attention_parts(kv_ref, jnp.maximum(me - count, 0), num_rows)
    attention_finish_block(state, v_block)
    attention_sum_block(state)
    attention_score_block(state, q_ref, k_block, bias_rows, False)


def attention_end(state, o_ref):
    raw_out = state[6][...]
    o_ref[...] = (
        raw_out * lax.rsqrt(jnp.mean(raw_out * raw_out, axis=1, keepdims=True) + norm_eps)
    ).astype(jnp.bfloat16)


def attention_state(num_rows, width):
    f32, bf16 = jnp.float32, jnp.bfloat16
    pieces = num_rows // 128
    return [
        pltpu.VMEM((num_rows, num_rows), f32),
        pltpu.VMEM((num_rows, num_rows), f32),
        pltpu.VMEM((pieces * num_rows, 256), f32),
        pltpu.VMEM((pieces * num_rows, 128), bf16),
        pltpu.VMEM((num_rows, num_rows), bf16),
        pltpu.VMEM((128, 256), bf16),
        pltpu.VMEM((num_rows, width), f32),
        pltpu.VMEM((num_rows, 128), f32),
    ]


def both_kernel(
    queries,
    keys,
    values,
    bias_rows,
    moe_in,
    gain,
    ids_across,
    mix_across,
    gate,
    up,
    down,
    shared_gate,
    shared_up,
    shared_down,
    heads,
    out,
    kv,
    turned,
    w_in,
    w_out,
    w_shared,
    cut,
    mixes,
    pre,
    outgoing,
    pooled,
    partial,
    inbox,
    result,
    shared_sum,
    returned,
    comb,
    cut_back,
    landed,
    w_sem,
    pre_send,
    pre_recv,
    mix_send,
    mix_recv,
    go_send,
    go_recv,
    ag_send,
    ag_recv,
    rs_send,
    rs_recv,
    back_send,
    back_recv,
    fin_send,
    fin_recv,
    up_send,
    up_recv,
    down_send,
    down_recv,
    pair_send,
    pair_recv,
    *state,
):
    ep_count, tp_count = lax.axis_size("ep"), 16
    rows = moe_in.shape[0]
    e = lax.axis_index("ep")
    y = lax.axis_index("tp_0")
    x = lax.axis_index("tp_1")
    t = y * 4 + x

    def tp_peer(k):
        other = lax.rem(t + k, tp_count)
        return other, {"tp_0": other // 4, "tp_1": lax.rem(other, 4)}

    barrier = pltpu.get_barrier_semaphore()

    def greet_tp(k, carry):
        pl.semaphore_signal(barrier, inc=1, device_id=tp_peer(k)[1], device_id_type=MESH)
        return carry

    def greet_ep(k, carry):
        pl.semaphore_signal(
            barrier, inc=1, device_id={"ep": lax.rem(e + k, ep_count)}, device_id_type=MESH
        )
        return carry

    lax.fori_loop(1, ep_count, greet_ep, 0)
    lax.fori_loop(1, tp_count, greet_tp, 0)

    loads = [
        pltpu.make_async_copy(gate, w_in.at[pl.ds(0, 2)], w_sem.at[0]),
        pltpu.make_async_copy(up, w_in.at[pl.ds(2, 2)], w_sem.at[1]),
        pltpu.make_async_copy(down, w_out, w_sem.at[2]),
        pltpu.make_async_copy(shared_gate, w_shared.at[0], w_sem.at[3]),
        pltpu.make_async_copy(shared_up, w_shared.at[1], w_sem.at[4]),
        pltpu.make_async_copy(shared_down, w_shared.at[2], w_sem.at[5]),
    ]
    for load in loads:
        load.start()

    as_float = moe_in[...].astype(jnp.float32)
    normed = (
        as_float
        * lax.rsqrt(jnp.mean(as_float * as_float, axis=1, keepdims=True) + norm_eps)
        * gain[...]
    ).astype(jnp.bfloat16)
    for k in range(tp_count):
        cut[k] = normed[:, k * 128 : (k + 1) * 128]
    top_k = ids_across.shape[0]
    turned[...] = jnp.zeros_like(turned)
    turned[0, :top_k, :] = ids_across[...].astype(jnp.float32)
    turned[1, :top_k, :rows] = mix_across[...]
    own_mix = turned[1].T[:rows, :]
    turned[0] = turned[0].T
    own_ids = turned[0, pl.ds(pl.multiple_of(t * rows, rows), rows), :]
    lane = lax.broadcasted_iota(jnp.int32, (rows, 128), 1).astype(jnp.float32)
    spread = jnp.zeros((rows, 128), jnp.float32)
    for k in range(top_k):
        spread = spread + jnp.where(own_ids[:, k : k + 1] == lane, own_mix[:, k : k + 1], 0.0)
    mixes[t] = spread
    pre[t] = cut[t]

    tokens = queries.shape[0]
    kv[e, :tokens, :] = keys[...]
    kv[e, tokens : 2 * tokens, :] = values[...]
    kv[e, 2 * tokens : 2 * tokens + 16, :] = bias_rows[...]
    attention_start(state, tokens)

    pl.semaphore_wait(barrier, ep_count + tp_count - 2)

    def send_pre(k, carry):
        other, device = tp_peer(k)
        pltpu.make_async_remote_copy(
            cut.at[other], pre.at[t], pre_send, pre_recv, device_id=device, device_id_type=MESH
        ).start()
        return carry

    def send_mix(k, carry):
        _, device = tp_peer(k)
        pltpu.make_async_remote_copy(
            mixes.at[t], mixes.at[t], mix_send, mix_recv, device_id=device, device_id_type=MESH
        ).start()
        return carry

    lax.fori_loop(1, tp_count, send_pre, 0)
    lax.fori_loop(1, tp_count, send_mix, 0)

    across = ids_across[...]
    expert_id = lax.broadcasted_iota(jnp.int32, (64, 128), 0)
    named = across[0:1] == expert_id
    for k in range(1, across.shape[0]):
        named = named | (across[k : k + 1] == expert_id)
    named = named.astype(jnp.float32)
    source = lax.broadcasted_iota(jnp.int32, (tp_count, 128), 0)
    same = (lax.broadcasted_iota(jnp.int32, (tp_count, 128), 1) // rows == source).astype(
        jnp.float32
    )
    for k in range(64):
        outgoing[k * 16 : (k + 1) * 16, :] = (same * named[k : k + 1, :]).astype(jnp.bfloat16)

    pltpu.make_async_copy(
        pre.at[pl.ds(0, tp_count - 1)], pre.at[pl.ds(0, tp_count - 1)], pre_recv
    ).wait()
    own_rows = pre[...].astype(jnp.float32).reshape(tp_count * rows, 128).astype(jnp.bfloat16)
    pooled[t, 1024:1152, :] = own_rows
    for k in range(4):
        part = slice(k * 256, (k + 1) * 256)
        outgoing[part, :] = jnp.dot(
            outgoing[part, :], own_rows, preferred_element_type=jnp.float32
        ).astype(jnp.bfloat16)
    at_e = pl.ds(pl.multiple_of(e * 32, 32), 32)

    def send_go(k, carry):
        other = lax.rem(e + k, ep_count)
        pltpu.make_async_remote_copy(
            outgoing.at[pl.ds(pl.multiple_of(other * 32, 32), 32)],
            pooled.at[t, at_e],
            go_send,
            go_recv,
            device_id={"ep": other},
            device_id_type=MESH,
        ).start()
        return carry

    lax.fori_loop(1, ep_count, send_go, 0)
    pooled[t, at_e, :] = outgoing[at_e, :]

    chips = ep_count // 2
    z, core = e // 2, lax.rem(e, 2)
    partner = e + 1 - 2 * core
    most_up, most_down = chips // 2, chips // 2 - 1

    def kv_copy(chip, target, send_sem, recv_sem):
        ref = kv.at[chip * 2 + core]
        return pltpu.make_async_remote_copy(
            ref, ref, send_sem, recv_sem, device_id={"ep": target}, device_id_type=MESH
        )

    def chip_at(step):
        return lax.rem(z + step + chips, chips)

    def up_copy(n):
        return kv_copy(
            chip_at(-n), chip_at(1) * 2 + core, up_send.at[n], up_recv.at[n + 1]
        )

    def down_copy(n):
        return kv_copy(
            chip_at(n), chip_at(-1) * 2 + core, down_send.at[n], down_recv.at[n + 1]
        )

    def pair_copy(chip):
        return kv_copy(chip, partner, pair_send.at[chip], pair_recv.at[chip])

    def goes_up(n):
        return (z - n >= 0) & (z < chips - 1)

    def goes_down(n):
        return chip_at(n) < most_down

    @pl.when(core == 0)
    def _():
        pair_copy(z).start()

    @pl.when(goes_up(0))
    def _():
        up_copy(0).start()

    @pl.when(goes_down(0))
    def _():
        down_copy(0).start()

    def kv_service(n):
        @pl.when(z >= n)
        def _():
            up_copy(n - 1).wait_recv()
            pair_copy(z - n).start()

        if n < most_up:

            @pl.when(goes_up(n))
            def _():
                up_copy(n).start()

        if n <= most_down:

            @pl.when(goes_down(n))
            def _():
                down_copy(n - 1).wait_recv()

                @pl.when(chip_at(n) < z)
                def _():
                    pair_copy(chip_at(n)).start()

                if n < most_down:
                    down_copy(n).start()

    def attend(first, last):
        def pair(n, carry):
            @pl.when(z >= n)
            def _():
                pair_wait(z - n)
                for extra in range(2):
                    attention_step(state, queries, kv, e, 2 * n - 1 + core + extra)

            return carry

        lax.fori_loop(first, last + 1, pair, 0)

    def pair_wait(chip):
        ref = kv.at[chip * 2 + 1 - core]
        pltpu.make_async_copy(ref, ref, pair_recv.at[chip]).wait()

    pltpu.make_async_copy(
        mixes.at[pl.ds(0, tp_count - 1)], mixes.at[pl.ds(0, tp_count - 1)], mix_recv
    ).wait()
    mix_all = mixes[...].reshape(tp_count * rows, 128)
    high = mix_all.astype(jnp.bfloat16)
    low = (mix_all - high.astype(jnp.float32)).astype(jnp.bfloat16)
    for k in range(4):
        column = k * 256 + lax.broadcasted_iota(jnp.int32, (128, 256), 1)
        row = lax.broadcasted_iota(jnp.int32, (128, 256), 0)
        widen = (column // 16 == row).astype(jnp.bfloat16)
        keep = lax.rem(column, 16) == row // rows
        for part, value in ((0, high), (1, low)):
            wide = jnp.dot(value, widen, preferred_element_type=jnp.float32)
            comb[part, :, k * 256 : (k + 1) * 256] = jnp.where(keep, wide, 0.0).astype(
                jnp.bfloat16
            )

    k_block, _, own_bias = attention_parts(kv, e, tokens)
    attention_score_block(state, queries, k_block, own_bias, True)

    pltpu.make_async_copy(
        pooled.at[t, pl.ds(0, 992)], pooled.at[t, pl.ds(0, 992)], go_recv
    ).wait()

    quarter = 288
    names = ("tp_0", "tp_1")
    place = {"tp_0": y, "tp_1": x}

    def axes(q):
        first, second = names if q < 2 else names[::-1]
        return first, second, 1 if q % 2 == 0 else 3

    def index_at(q, df, dg):
        first, second, _ = axes(q)
        moved = {
            first: lax.rem(place[first] + df % 4, 4),
            second: lax.rem(place[second] + dg % 4, 4),
        }
        return moved["tp_0"] * 4 + moved["tp_1"]

    def block(ref, q, df, dg):
        return ref.at[index_at(q, df, dg), pl.ds(q * quarter, quarter)]

    def ag_copy(q, df, dg, along_first, step):
        first, second, _ = axes(q)
        axis = first if along_first else second
        there = ((df - step) % 4, dg % 4) if along_first else (df % 4, (dg - step) % 4)
        ref = block(pooled, q, df, dg)
        return pltpu.make_async_remote_copy(
            ref,
            ref,
            ag_send,
            ag_recv.at[q, there[0] * 4 + there[1]],
            device_id={axis: lax.rem(place[axis] + step % 4, 4)},
            device_id_type=MESH,
        )

    def ag_wait(q, df, dg):
        ref = block(pooled, q, df, dg)
        pltpu.make_async_copy(ref, ref, ag_recv.at[q, (df % 4) * 4 + dg % 4]).wait()

    quarters = range(4)
    for q in quarters:
        ag_copy(q, 0, 0, True, 1).start()
        ag_copy(q, 0, 0, True, 3).start()
    for q in quarters:
        ag_copy(q, 0, 0, False, 1).start()
        ag_copy(q, 0, 0, False, 3).start()
    for q in quarters:
        d = axes(q)[2]
        ag_wait(q, -d, 0)
        ag_copy(q, -d, 0, True, d).start()
        ag_copy(q, -d, 0, False, 1).start()
        ag_copy(q, -d, 0, False, 3).start()
    for q in quarters:
        d = axes(q)[2]
        ag_wait(q, d, 0)
        ag_copy(q, d, 0, False, 1).start()
        ag_copy(q, d, 0, False, 3).start()
    for q in quarters:
        d = axes(q)[2]
        ag_wait(q, 0, -d)
        ag_copy(q, 0, -d, False, d).start()
    for q in quarters:
        ag_wait(q, 2, 0)
        ag_copy(q, 2, 0, False, 1).start()
        ag_copy(q, 2, 0, False, 3).start()
    kv_service(1)

    @pl.when(core == 1)
    def _():
        pair_wait(z)
        attention_step(state, queries, kv, e, 1)

    for hop in range(3):
        for q in quarters:
            d = axes(q)[2]
            df = (-d, d, 2)[hop]
            ag_wait(q, df, -d)
            ag_copy(q, df, -d, False, d).start()
        if hop > 0:
            kv_service(hop + 1)

    for load in loads:
        load.wait()

    def rs_copy(q, ref, slot, along_first, step):
        first, second, _ = axes(q)
        axis = first if along_first else second
        return pltpu.make_async_remote_copy(
            ref,
            inbox.at[q, slot],
            rs_send,
            rs_recv.at[q, slot],
            device_id={axis: lax.rem(place[axis] + step % 4, 4)},
            device_id_type=MESH,
        )

    def rs_wait(q, slot):
        ref = inbox.at[q, slot]
        pltpu.make_async_copy(ref, ref, rs_recv.at[q, slot]).wait()

    def plus(q, df, dg, *slots):
        where = index_at(q, df, dg)
        total = partial[where, q * quarter : (q + 1) * quarter, :].astype(jnp.float32)
        for slot in slots:
            total = total + inbox[q, slot].astype(jnp.float32)
        return where, total

    def silu_times(both):
        half = both.shape[1] // 2
        gate_val = both[:, :half]
        return gate_val * (1.0 / (1.0 + jnp.exp(-gate_val))) * both[:, half:]

    def feed(span, weights_in, weights_out, routed):
        both = jnp.concatenate([pooled[k, span, :] for k in range(tp_count)], axis=1)
        hidden = silu_times(
            lax.dot_general(
                both, weights_in, (((1,), (1,)), ((), ())), preferred_element_type=jnp.float32
            )
        )
        if routed:
            row = lax.broadcasted_iota(jnp.int32, hidden.shape, 0)
            column = lax.broadcasted_iota(jnp.int32, hidden.shape, 1)
            hidden = jnp.where(lax.rem(row // 16, 2) == column // 64, hidden, 0.0)
        hidden = hidden.astype(jnp.bfloat16)
        for k in range(0, tp_count, 2):
            term = jnp.dot(
                hidden,
                weights_out[:, k * 128 : (k + 2) * 128],
                preferred_element_type=jnp.float32,
            ).astype(jnp.bfloat16)
            partial[k, span, :] = term[:, :128]
            partial[k + 1, span, :] = term[:, 128:]

    for q in quarters:
        d = axes(q)[2]
        for df in range(4):
            ag_wait(q, df, d)
            ag_wait(q, df, 2)
        last = q == 3
        span = slice(q * quarter, 1024 if last else (q + 1) * quarter)
        feed(span, w_in[...].reshape(256, 2048), w_out[...].reshape(128, 2048), True)
        if last:
            feed(
                slice(1024, 1152), w_shared[0:2].reshape(128, 2048), w_shared[2], False
            )
        for df in (2, -d, d, 0):
            slot = (df % 4) * 3
            rs_copy(q, block(partial, q, df, 2), slot, False, d).start()
            rs_copy(q, block(partial, q, df, -d), slot + 1, False, -d).start()

    kv_service(4)
    attend(1, 3)
    kv_service(5)
    attend(4, 4)
    rows_of = lambda q: slice(q * quarter, (q + 1) * quarter)
    for turn in range(4):
        for q in quarters:
            d = axes(q)[2]
            df = (2, -d, d, 0)[turn] % 4
            rs_wait(q, df * 3)
            where, total = plus(q, df, d, df * 3)
            partial[where, rows_of(q), :] = total.astype(jnp.bfloat16)
            rs_copy(q, block(partial, q, df, d), df * 3 + 2, False, d).start()
        if turn < 3:
            kv_service(turn + 6)
        attend(turn + 5, turn + 5)
    for turn in range(4):
        for q in quarters:
            d = axes(q)[2]
            df = (2, -d, d, 0)[turn] % 4
            rs_wait(q, df * 3 + 1)
            rs_wait(q, df * 3 + 2)
            slots = [df * 3 + 1, df * 3 + 2]
            if turn == 2:
                rs_wait(q, 12)
                slots.append(12)
            where, total = plus(q, df, 0, *slots)
            partial[where, rows_of(q), :] = total.astype(jnp.bfloat16)
            if turn == 0:
                rs_copy(q, block(partial, q, df, 0), 12, True, d).start()
            elif turn == 1:
                rs_copy(q, block(partial, q, df, 0), 13, True, -d).start()
            elif turn == 2:
                rs_copy(q, block(partial, q, df, 0), 14, True, d).start()
        if turn < 3:
            attend(turn + 9, turn + 9)

    for q in quarters:
        rs_wait(q, 13)
        rs_wait(q, 14)
        _, total = plus(q, 0, 0, 13, 14)
        result[rows_of(q), :] = total.astype(jnp.bfloat16)
        if q == 3:
            shared_sum[...] = total[160:288, :]

        def send_back(other, carry):
            @pl.when(other != e)
            def _():
                pltpu.make_async_remote_copy(
                    result.at[pl.ds(pl.multiple_of(other * 32, 32), 32)],
                    returned.at[at_e],
                    back_send,
                    back_recv,
                    device_id={"ep": other},
                    device_id_type=MESH,
                ).start()

            return carry

        lax.fori_loop(q * 9, min(ep_count, (q + 1) * 9), send_back, 0)
    returned[at_e, :] = result[at_e, :]
    attend(12, chips - 1)
    for extra in range(2):
        attention_step(state, queries, kv, e, e + 1 + extra)
    attention_end(state, heads)
    pltpu.make_async_copy(
        returned.at[pl.ds(0, 992)], returned.at[pl.ds(0, 992)], back_recv
    ).wait()
    combined = (
        shared_sum[...]
        + jnp.dot(comb[0], returned[...], preferred_element_type=jnp.float32)
        + jnp.dot(comb[1], returned[...], preferred_element_type=jnp.float32)
    )
    for k in range(tp_count):
        cut_back[k] = combined[k * rows : (k + 1) * rows, :].astype(jnp.bfloat16)

    def send_fin(k, carry):
        other, device = tp_peer(k)
        pltpu.make_async_remote_copy(
            cut_back.at[other],
            landed.at[t],
            fin_send,
            fin_recv,
            device_id=device,
            device_id_type=MESH,
        ).start()
        return carry

    lax.fori_loop(1, tp_count, send_fin, 0)
    landed[t] = cut_back[t]

    most = tp_count - 1
    for ref, sem in (
        (pre.at[pl.ds(0, most)], pre_send),
        (mixes.at[pl.ds(0, most)], mix_send),
        (outgoing.at[pl.ds(0, 992)], go_send),
        (pooled.at[pl.ds(0, most)], ag_send),
        (partial.at[pl.ds(0, most)], rs_send),
        (result.at[pl.ds(0, 992)], back_send),
        (landed.at[pl.ds(0, most)], fin_recv),
        (landed.at[pl.ds(0, most)], fin_send),
    ):
        pltpu.make_async_copy(ref, ref, sem).wait()

    @pl.when(core == 0)
    def _():
        pair_copy(z).wait_send()

    for n in range(most_up):

        @pl.when(goes_up(n))
        def _():
            up_copy(n).wait_send()

    for n in range(most_down):

        @pl.when(goes_down(n))
        def _():
            down_copy(n).wait_send()

    for n in range(1, chips):

        @pl.when(z >= n)
        def _():
            pair_copy(z - n).wait_send()

    for k in range(tp_count):
        out[:, k * 128 : (k + 1) * 128] = landed[k]


def both_halves(
    queries,
    keys,
    values,
    key_bias,
    moe_in,
    norm_gain,
    route_ids,
    route_weights,
    gate_weight,
    up_weight,
    down_weight,
    shared_gate,
    shared_up,
    shared_down,
):
    own_rows, width = moe_in.shape
    tokens, head_dim = queries.shape
    bias_rows = key_bias.reshape(tokens // head_dim, head_dim)
    bias_rows = jnp.pad(bias_rows, ((0, 16 - tokens // head_dim), (0, 0)))
    hidden = gate_weight.shape[1]
    bf16, f32 = jnp.bfloat16, jnp.float32
    vmem, dma = pltpu.VMEM, pltpu.SemaphoreType.DMA
    here, there = pl.BlockSpec(memory_space=pltpu.VMEM), pl.BlockSpec(memory_space=pl.ANY)
    return pl.pallas_call(
        both_kernel,
        out_shape=(
            jax.ShapeDtypeStruct((tokens, head_dim), bf16),
            jax.ShapeDtypeStruct((own_rows, width), bf16),
        ),
        in_specs=[here] * 8 + [there] * 6,
        out_specs=(here, here),
        scratch_shapes=[
            vmem((32, 2 * tokens + 16, head_dim), bf16),
            vmem((2, 128, 128), f32),
            vmem((4, hidden, width), bf16),
            vmem((2, hidden, width), bf16),
            vmem((3, hidden, width), bf16),
            vmem((16, own_rows, 128), bf16),
            vmem((16, own_rows, 128), f32),
            vmem((16, own_rows, 128), bf16),
            vmem((1024, 128), bf16),
            vmem((16, 1152, 128), bf16),
            vmem((16, 1152, 128), bf16),
            vmem((4, 15, 288, 128), bf16),
            vmem((1152, 128), bf16),
            vmem((128, 128), f32),
            vmem((1024, 128), bf16),
            vmem((2, 128, 1024), bf16),
            vmem((16, own_rows, 128), bf16),
            vmem((16, own_rows, 128), bf16),
            dma((6,)),
            dma,
            dma,
            dma,
            dma,
            dma,
            dma,
            dma,
            dma((4, 16)),
            dma,
            dma((4, 15)),
            dma,
            dma,
            dma,
            dma,
            dma((8,)),
            dma((9,)),
            dma((8,)),
            dma((9,)),
            dma((16,)),
            dma((16,)),
            *attention_state(tokens, head_dim),
        ],
        compiler_params=pltpu.CompilerParams(
            collective_id=0, has_side_effects=True, vmem_limit_bytes=60 * 1024 * 1024
        ),
        cost_estimate=pl.CostEstimate(
            flops=80_000_000_000, bytes_accessed=200_000_000, transcendentals=300_000
        ),
    )(
        queries,
        keys,
        values,
        bias_rows,
        moe_in,
        norm_gain[None, :],
        route_ids.T,
        route_weights.T,
        gate_weight,
        up_weight,
        down_weight,
        shared_gate,
        shared_up,
        shared_down,
    )


def shards(
    queries,
    keys,
    values,
    key_bias,
    moe_in,
    norm_gain,
    route_ids,
    route_weights,
    gate_weight,
    up_weight,
    down_weight,
    shared_gate,
    shared_up,
    shared_down,
):
    return both_halves(
        queries,
        keys,
        values,
        key_bias,
        moe_in,
        norm_gain,
        route_ids,
        route_weights,
        gate_weight,
        up_weight,
        down_weight,
        shared_gate,
        shared_up,
        shared_down,
    )


def solution(mesh):
    split = Mesh(mesh.devices.reshape(mesh.shape["ep"], 4, 4), ("ep", "tp_0", "tp_1"))
    return jax.shard_map(
        shards,
        mesh=split,
        in_specs=(
            P("ep", TP),
            P("ep", TP),
            P("ep", TP),
            P("ep", TP),
            P(EP_TP, None),
            P(),
            P("ep", None),
            P(EP_TP, None),
            P("ep", TP, None),
            P("ep", TP, None),
            P("ep", TP, None),
            P(TP, None),
            P(TP, None),
            P(TP, None),
        ),
        out_specs=(P("ep", TP), P(EP_TP, None)),
        check_vma=False,
    )
```

```python
import functools

import jax
import jax.numpy as jnp
from jax import lax
from jax.experimental import pallas as pl
from jax.experimental.pallas import tpu as pltpu
from jax.sharding import Mesh
from jax.sharding import PartitionSpec as P

TP = ("tp_0", "tp_1")
EP_TP = ("ep", "tp_0", "tp_1")


norm_eps = 1e-05
MESH = pl.DeviceIdType.MESH


FAR = -1e30


def attention_start(state, row_count):
    scores_ref, logit_ref, sums_ref, soft_ref, weight_ref, tri, acc, later = state
    row_id = lax.broadcasted_iota(jnp.int32, tri.shape, 0)
    col_id = lax.broadcasted_iota(jnp.int32, tri.shape, 1)
    tri[...] = jnp.where((row_id > col_id) | (col_id >= 128), -1.0, 0.0).astype(jnp.bfloat16)
    acc[...] = jnp.zeros_like(acc)
    later[...] = jnp.zeros_like(later)
    sums_ref[...] = jnp.zeros_like(sums_ref)
    logit_ref[...] = jnp.full(logit_ref.shape, FAR, jnp.float32)
    scores_ref[...] = jnp.full(scores_ref.shape, FAR, jnp.float32)


def attention_finish_block(state, v_block):
    scores_ref, logit_ref, sums_ref, soft_ref, weight_ref, tri, acc, later = state
    num_rows = scores_ref.shape[0]
    piece = 16
    for first in range(0, num_rows, piece):
        carried = later[first : first + piece, :]
        for c in reversed(range(num_rows // 128)):
            at = c * num_rows + first
            weight_ref[first : first + piece, c * 128 : (c + 1) * 128] = jnp.exp(
                logit_ref[first : first + piece, c * 128 : (c + 1) * 128]
                + (sums_ref[at : at + piece, :128] + carried)
            ).astype(jnp.bfloat16)
            carried = carried + sums_ref[at : at + piece, 128:]
        later[first : first + piece, :] = carried
    acc[...] += jnp.dot(weight_ref[...], v_block, preferred_element_type=jnp.float32)


def attention_sum_block(state):
    scores_ref, logit_ref, sums_ref, soft_ref, weight_ref, tri, acc, later = state
    num_rows = scores_ref.shape[0]
    piece = 16
    for c in range(num_rows // 128):
        columns = slice(c * 128, (c + 1) * 128)
        for first in range(0, num_rows, piece):
            scores = scores_ref[first : first + piece, columns]
            soft = jnp.maximum(scores, jnp.log(1.0 + jnp.exp(jnp.minimum(scores, 88.0))))
            logit_ref[first : first + piece, columns] = scores - soft
            soft_ref[c * num_rows + first : c * num_rows + first + piece, :] = soft.astype(
                jnp.bfloat16
            )
    sums_ref[...] = jnp.dot(soft_ref[...], tri[...], preferred_element_type=jnp.float32)


def attention_score_block(state, q_ref, k_block, bias_rows, diagonal):
    scores_ref = state[0]
    num_rows, width = q_ref.shape
    bias = bias_rows.astype(jnp.float32)
    bias = jnp.concatenate([bias[r : r + 1] for r in range(num_rows // width)], axis=1)
    products = lax.dot_general(
        q_ref[...], k_block, (((1,), (1,)), ((), ())), preferred_element_type=jnp.float32
    )
    scores = products * width ** (-0.5) + bias
    if diagonal:
        causal = lax.broadcasted_iota(jnp.int32, scores.shape, 1) < lax.broadcasted_iota(
            jnp.int32, scores.shape, 0
        )
        scores = jnp.where(causal, scores, FAR)
    scores_ref[...] = scores


def attention_parts(kv_ref, block, num_rows):
    return (
        kv_ref[block, :num_rows, :],
        kv_ref[block, num_rows : 2 * num_rows, :],
        kv_ref[block, 2 * num_rows : 2 * num_rows + 16, :],
    )


def attention_step(state, q_ref, kv_ref, me, count):
    num_rows = q_ref.shape[0]
    v_block = attention_parts(kv_ref, jnp.minimum(me - count + 2, me), num_rows)[1]
    k_block, _, bias_rows = attention_parts(kv_ref, jnp.maximum(me - count, 0), num_rows)
    attention_finish_block(state, v_block)
    attention_sum_block(state)
    attention_score_block(state, q_ref, k_block, bias_rows, False)


def attention_end(state, o_ref):
    raw_out = state[6][...]
    o_ref[...] = (
        raw_out * lax.rsqrt(jnp.mean(raw_out * raw_out, axis=1, keepdims=True) + norm_eps)
    ).astype(jnp.bfloat16)


def attention_state(num_rows, width):
    f32, bf16 = jnp.float32, jnp.bfloat16
    pieces = num_rows // 128
    return [
        pltpu.VMEM((num_rows, num_rows), f32),
        pltpu.VMEM((num_rows, num_rows), f32),
        pltpu.VMEM((pieces * num_rows, 256), f32),
        pltpu.VMEM((pieces * num_rows, 128), bf16),
        pltpu.VMEM((num_rows, num_rows), bf16),
        pltpu.VMEM((128, 256), bf16),
        pltpu.VMEM((num_rows, width), f32),
        pltpu.VMEM((num_rows, 128), f32),
    ]


def both_kernel(
    queries,
    keys,
    values,
    bias_rows,
    moe_in,
    gain,
    ids_across,
    mix_across,
    gate,
    up,
    down,
    shared_gate,
    shared_up,
    shared_down,
    heads,
    out,
    kv,
    turned,
    w_in,
    w_out,
    w_shared,
    cut,
    mixes,
    pre,
    outgoing,
    pooled,
    partial,
    inbox,
    result,
    shared_sum,
    returned,
    comb,
    cut_back,
    landed,
    w_sem,
    pre_send,
    pre_recv,
    mix_send,
    mix_recv,
    go_send,
    go_recv,
    ag_send,
    ag_recv,
    rs_send,
    rs_recv,
    back_send,
    back_recv,
    fin_send,
    fin_recv,
    up_send,
    up_recv,
    down_send,
    down_recv,
    pair_send,
    pair_recv,
    *state,
):
    ep_count, tp_count = lax.axis_size("ep"), 16
    rows = moe_in.shape[0]
    e = lax.axis_index("ep")
    y = lax.axis_index("tp_0")
    x = lax.axis_index("tp_1")
    t = y * 4 + x

    def tp_peer(k):
        other = lax.rem(t + k, tp_count)
        return other, {"tp_0": other // 4, "tp_1": lax.rem(other, 4)}

    barrier = pltpu.get_barrier_semaphore()

    def greet_tp(k, carry):
        pl.semaphore_signal(barrier, inc=1, device_id=tp_peer(k)[1], device_id_type=MESH)
        return carry

    def greet_ep(k, carry):
        pl.semaphore_signal(
            barrier, inc=1, device_id={"ep": lax.rem(e + k, ep_count)}, device_id_type=MESH
        )
        return carry

    lax.fori_loop(1, ep_count, greet_ep, 0)
    lax.fori_loop(1, tp_count, greet_tp, 0)

    loads = [
        pltpu.make_async_copy(gate, w_in.at[pl.ds(0, 2)], w_sem.at[0]),
        pltpu.make_async_copy(up, w_in.at[pl.ds(2, 2)], w_sem.at[1]),
        pltpu.make_async_copy(down, w_out, w_sem.at[2]),
        pltpu.make_async_copy(shared_gate, w_shared.at[0], w_sem.at[3]),
        pltpu.make_async_copy(shared_up, w_shared.at[1], w_sem.at[4]),
        pltpu.make_async_copy(shared_down, w_shared.at[2], w_sem.at[5]),
    ]
    for load in loads:
        load.start()

    as_float = moe_in[...].astype(jnp.float32)
    normed = (
        as_float
        * lax.rsqrt(jnp.mean(as_float * as_float, axis=1, keepdims=True) + norm_eps)
        * gain[...]
    ).astype(jnp.bfloat16)
    for k in range(tp_count):
        cut[k] = normed[:, k * 128 : (k + 1) * 128]
    top_k = ids_across.shape[0]
    turned[...] = jnp.zeros_like(turned)
    turned[0, :top_k, :] = ids_across[...].astype(jnp.float32)
    turned[1, :top_k, :rows] = mix_across[...]
    own_mix = turned[1].T[:rows, :]
    turned[0] = turned[0].T
    own_ids = turned[0, pl.ds(pl.multiple_of(t * rows, rows), rows), :]
    lane = lax.broadcasted_iota(jnp.int32, (rows, 128), 1).astype(jnp.float32)
    spread = jnp.zeros((rows, 128), jnp.float32)
    for k in range(top_k):
        spread = spread + jnp.where(own_ids[:, k : k + 1] == lane, own_mix[:, k : k + 1], 0.0)
    mixes[t] = spread
    pre[t] = cut[t]

    tokens = queries.shape[0]
    kv[e, :tokens, :] = keys[...]
    kv[e, tokens : 2 * tokens, :] = values[...]
    kv[e, 2 * tokens : 2 * tokens + 16, :] = bias_rows[...]
    attention_start(state, tokens)

    pl.semaphore_wait(barrier, ep_count + tp_count - 2)

    chips = ep_count // 2
    z, core = e // 2, lax.rem(e, 2)
    partner = e + 1 - 2 * core
    most_up, most_down = chips // 2, chips // 2 - 1

    def kv_copy(chip, target, send_sem, recv_sem):
        ref = kv.at[chip * 2 + core]
        return pltpu.make_async_remote_copy(
            ref, ref, send_sem, recv_sem, device_id={"ep": target}, device_id_type=MESH
        )

    def chip_at(step):
        return lax.rem(z + step + chips, chips)

    def up_copy(n):
        return kv_copy(
            chip_at(-n), chip_at(1) * 2 + core, up_send.at[n], up_recv.at[n + 1]
        )

    def down_copy(n):
        return kv_copy(
            chip_at(n), chip_at(-1) * 2 + core, down_send.at[n], down_recv.at[n + 1]
        )

    def pair_copy(chip):
        return kv_copy(chip, partner, pair_send.at[chip], pair_recv.at[chip])

    def goes_up(n):
        return (z - n >= 0) & (z < chips - 1)

    def goes_down(n):
        return chip_at(n) < most_down

    def kv_service(n):
        @pl.when(z >= n)
        def _():
            up_copy(n - 1).wait_recv()
            pair_copy(z - n).start()

        if n < most_up:

            @pl.when(goes_up(n))
            def _():
                up_copy(n).start()

        if n <= most_down:

            @pl.when(goes_down(n))
            def _():
                down_copy(n - 1).wait_recv()

                @pl.when(chip_at(n) < z)
                def _():
                    pair_copy(chip_at(n)).start()

                if n < most_down:
                    down_copy(n).start()

    def attend(first, last):
        def pair(n, carry):
            @pl.when(z >= n)
            def _():
                pair_wait(z - n)
                for extra in range(2):
                    attention_step(state, queries, kv, e, 2 * n - 1 + core + extra)

            return carry

        lax.fori_loop(first, last + 1, pair, 0)

    def pair_wait(chip):
        ref = kv.at[chip * 2 + 1 - core]
        pltpu.make_async_copy(ref, ref, pair_recv.at[chip]).wait()


    def send_pre(k, carry):
        other, device = tp_peer(k)
        pltpu.make_async_remote_copy(
            cut.at[other], pre.at[t], pre_send, pre_recv, device_id=device, device_id_type=MESH
        ).start()
        return carry

    def send_mix(k, carry):
        _, device = tp_peer(k)
        pltpu.make_async_remote_copy(
            mixes.at[t], mixes.at[t], mix_send, mix_recv, device_id=device, device_id_type=MESH
        ).start()
        return carry

    lax.fori_loop(1, tp_count, send_pre, 0)

    @pl.when(core == 0)
    def _():
        pair_copy(z).start()

    @pl.when(goes_up(0))
    def _():
        up_copy(0).start()

    @pl.when(goes_down(0))
    def _():
        down_copy(0).start()


    across = ids_across[...]
    expert_id = lax.broadcasted_iota(jnp.int32, (64, 128), 0)
    named = across[0:1] == expert_id
    for k in range(1, across.shape[0]):
        named = named | (across[k : k + 1] == expert_id)
    named = named.astype(jnp.float32)
    source = lax.broadcasted_iota(jnp.int32, (tp_count, 128), 0)
    same = (lax.broadcasted_iota(jnp.int32, (tp_count, 128), 1) // rows == source).astype(
        jnp.float32
    )
    for k in range(64):
        outgoing[k * 16 : (k + 1) * 16, :] = (same * named[k : k + 1, :]).astype(jnp.bfloat16)

    pltpu.make_async_copy(
        pre.at[pl.ds(0, tp_count - 1)], pre.at[pl.ds(0, tp_count - 1)], pre_recv
    ).wait()
    own_rows = pre[...].astype(jnp.float32).reshape(tp_count * rows, 128).astype(jnp.bfloat16)
    pooled[t, 1024:1152, :] = own_rows
    for k in range(4):
        part = slice(k * 256, (k + 1) * 256)
        outgoing[part, :] = jnp.dot(
            outgoing[part, :], own_rows, preferred_element_type=jnp.float32
        ).astype(jnp.bfloat16)
    at_e = pl.ds(pl.multiple_of(e * 32, 32), 32)

    def send_go(k, carry):
        other = lax.rem(e + k, ep_count)
        pltpu.make_async_remote_copy(
            outgoing.at[pl.ds(pl.multiple_of(other * 32, 32), 32)],
            pooled.at[t, at_e],
            go_send,
            go_recv,
            device_id={"ep": other},
            device_id_type=MESH,
        ).start()
        return carry

    lax.fori_loop(1, ep_count, send_go, 0)
    lax.fori_loop(1, tp_count, send_mix, 0)
    pooled[t, at_e, :] = outgoing[at_e, :]
    kv_service(1)
    k_block, _, own_bias = attention_parts(kv, e, tokens)
    attention_score_block(state, queries, k_block, own_bias, True)

    @pl.when(core == 1)
    def _():
        pair_wait(z)
        attention_step(state, queries, kv, e, 1)

    attend(1, 1)

    pltpu.make_async_copy(
        mixes.at[pl.ds(0, tp_count - 1)], mixes.at[pl.ds(0, tp_count - 1)], mix_recv
    ).wait()
    mix_all = mixes[...].reshape(tp_count * rows, 128)
    high = mix_all.astype(jnp.bfloat16)
    low = (mix_all - high.astype(jnp.float32)).astype(jnp.bfloat16)
    for k in range(4):
        column = k * 256 + lax.broadcasted_iota(jnp.int32, (128, 256), 1)
        row = lax.broadcasted_iota(jnp.int32, (128, 256), 0)
        widen = (column // 16 == row).astype(jnp.bfloat16)
        keep = lax.rem(column, 16) == row // rows
        for part, value in ((0, high), (1, low)):
            wide = jnp.dot(value, widen, preferred_element_type=jnp.float32)
            comb[part, :, k * 256 : (k + 1) * 256] = jnp.where(keep, wide, 0.0).astype(
                jnp.bfloat16
            )

    pltpu.make_async_copy(
        pooled.at[t, pl.ds(0, 992)], pooled.at[t, pl.ds(0, 992)], go_recv
    ).wait()

    quarter = 288
    names = ("tp_0", "tp_1")
    place = {"tp_0": y, "tp_1": x}

    def axes(q):
        first, second = names if q < 2 else names[::-1]
        return first, second, 1 if q % 2 == 0 else 3

    def index_at(q, df, dg):
        first, second, _ = axes(q)
        moved = {
            first: lax.rem(place[first] + df % 4, 4),
            second: lax.rem(place[second] + dg % 4, 4),
        }
        return moved["tp_0"] * 4 + moved["tp_1"]

    def block(ref, q, df, dg):
        return ref.at[index_at(q, df, dg), pl.ds(q * quarter, quarter)]

    def ag_copy(q, df, dg, along_first, step):
        first, second, _ = axes(q)
        axis = first if along_first else second
        there = ((df - step) % 4, dg % 4) if along_first else (df % 4, (dg - step) % 4)
        ref = block(pooled, q, df, dg)
        return pltpu.make_async_remote_copy(
            ref,
            ref,
            ag_send,
            ag_recv.at[q, there[0] * 4 + there[1]],
            device_id={axis: lax.rem(place[axis] + step % 4, 4)},
            device_id_type=MESH,
        )

    def ag_wait(q, df, dg):
        ref = block(pooled, q, df, dg)
        pltpu.make_async_copy(ref, ref, ag_recv.at[q, (df % 4) * 4 + dg % 4]).wait()

    quarters = range(4)
    for q in quarters:
        ag_copy(q, 0, 0, True, 1).start()
        ag_copy(q, 0, 0, True, 3).start()
    for q in quarters:
        ag_copy(q, 0, 0, False, 1).start()
        ag_copy(q, 0, 0, False, 3).start()
    for q in quarters:
        d = axes(q)[2]
        ag_wait(q, -d, 0)
        ag_copy(q, -d, 0, True, d).start()
        ag_copy(q, -d, 0, False, 1).start()
        ag_copy(q, -d, 0, False, 3).start()
    kv_service(2)
    for q in quarters:
        d = axes(q)[2]
        ag_wait(q, d, 0)
        ag_copy(q, d, 0, False, 1).start()
        ag_copy(q, d, 0, False, 3).start()
    for q in quarters:
        d = axes(q)[2]
        ag_wait(q, 0, -d)
        ag_copy(q, 0, -d, False, d).start()
    for q in quarters:
        ag_wait(q, 2, 0)
        ag_copy(q, 2, 0, False, 1).start()
        ag_copy(q, 2, 0, False, 3).start()
        if q == 1:
            kv_service(3)
    for hop in range(3):
        for q in quarters:
            d = axes(q)[2]
            df = (-d, d, 2)[hop]
            ag_wait(q, df, -d)
            ag_copy(q, df, -d, False, d).start()
            if hop == 1 and q == 1:
                kv_service(4)
    attend(2, 2)
    kv_service(5)
    attend(3, 3)

    for load in loads:
        load.wait()

    def rs_copy(q, ref, slot, along_first, step):
        first, second, _ = axes(q)
        axis = first if along_first else second
        return pltpu.make_async_remote_copy(
            ref,
            inbox.at[q, slot],
            rs_send,
            rs_recv.at[q, slot],
            device_id={axis: lax.rem(place[axis] + step % 4, 4)},
            device_id_type=MESH,
        )

    def rs_wait(q, slot):
        ref = inbox.at[q, slot]
        pltpu.make_async_copy(ref, ref, rs_recv.at[q, slot]).wait()

    def plus(q, df, dg, *slots):
        where = index_at(q, df, dg)
        total = partial[where, q * quarter : (q + 1) * quarter, :].astype(jnp.float32)
        for slot in slots:
            total = total + inbox[q, slot].astype(jnp.float32)
        return where, total

    def silu_times(both):
        half = both.shape[1] // 2
        gate_val = both[:, :half]
        return gate_val * (1.0 / (1.0 + jnp.exp(-gate_val))) * both[:, half:]

    def feed(span, weights_in, weights_out, routed):
        both = jnp.concatenate([pooled[k, span, :] for k in range(tp_count)], axis=1)
        hidden = silu_times(
            lax.dot_general(
                both, weights_in, (((1,), (1,)), ((), ())), preferred_element_type=jnp.float32
            )
        )
        if routed:
            row = lax.broadcasted_iota(jnp.int32, hidden.shape, 0)
            column = lax.broadcasted_iota(jnp.int32, hidden.shape, 1)
            hidden = jnp.where(lax.rem(row // 16, 2) == column // 64, hidden, 0.0)
        hidden = hidden.astype(jnp.bfloat16)
        for k in range(0, tp_count, 2):
            term = jnp.dot(
                hidden,
                weights_out[:, k * 128 : (k + 2) * 128],
                preferred_element_type=jnp.float32,
            ).astype(jnp.bfloat16)
            partial[k, span, :] = term[:, :128]
            partial[k + 1, span, :] = term[:, 128:]

    for q in quarters:
        d = axes(q)[2]
        for df in range(4):
            ag_wait(q, df, d)
            ag_wait(q, df, 2)
        last = q == 3
        span = slice(q * quarter, 1024 if last else (q + 1) * quarter)
        feed(span, w_in[...].reshape(256, 2048), w_out[...].reshape(128, 2048), True)
        if last:
            feed(
                slice(1024, 1152), w_shared[0:2].reshape(128, 2048), w_shared[2], False
            )
        for df in (2, -d, d, 0):
            slot = (df % 4) * 3
            rs_copy(q, block(partial, q, df, 2), slot, False, d).start()
            rs_copy(q, block(partial, q, df, -d), slot + 1, False, -d).start()
        if q == 1:
            kv_service(6)

    attend(4, 5)
    rows_of = lambda q: slice(q * quarter, (q + 1) * quarter)
    for turn in range(4):
        for q in quarters:
            d = axes(q)[2]
            df = (2, -d, d, 0)[turn] % 4
            rs_wait(q, df * 3)
            where, total = plus(q, df, d, df * 3)
            partial[where, rows_of(q), :] = total.astype(jnp.bfloat16)
            rs_copy(q, block(partial, q, df, d), df * 3 + 2, False, d).start()
        if turn < 2:
            kv_service(turn + 7)
        attend(turn + 6, turn + 6)
    for turn in range(4):
        for q in quarters:
            d = axes(q)[2]
            df = (2, -d, d, 0)[turn] % 4
            rs_wait(q, df * 3 + 1)
            rs_wait(q, df * 3 + 2)
            slots = [df * 3 + 1, df * 3 + 2]
            if turn == 2:
                rs_wait(q, 12)
                slots.append(12)
            where, total = plus(q, df, 0, *slots)
            partial[where, rows_of(q), :] = total.astype(jnp.bfloat16)
            if turn == 0:
                rs_copy(q, block(partial, q, df, 0), 12, True, d).start()
            elif turn == 1:
                rs_copy(q, block(partial, q, df, 0), 13, True, -d).start()
            elif turn == 2:
                rs_copy(q, block(partial, q, df, 0), 14, True, d).start()
        if turn < 3:
            attend(turn + 10, turn + 10)

    for q in quarters:
        rs_wait(q, 13)
        rs_wait(q, 14)
        _, total = plus(q, 0, 0, 13, 14)
        result[rows_of(q), :] = total.astype(jnp.bfloat16)
        if q == 3:
            shared_sum[...] = total[160:288, :]

        def send_back(other, carry):
            @pl.when(other != e)
            def _():
                pltpu.make_async_remote_copy(
                    result.at[pl.ds(pl.multiple_of(other * 32, 32), 32)],
                    returned.at[at_e],
                    back_send,
                    back_recv,
                    device_id={"ep": other},
                    device_id_type=MESH,
                ).start()

            return carry

        lax.fori_loop(q * 9, min(ep_count, (q + 1) * 9), send_back, 0)
    returned[at_e, :] = result[at_e, :]
    attend(13, chips - 1)
    for extra in range(2):
        attention_step(state, queries, kv, e, e + 1 + extra)
    attention_end(state, heads)
    pltpu.make_async_copy(
        returned.at[pl.ds(0, 992)], returned.at[pl.ds(0, 992)], back_recv
    ).wait()
    combined = (
        shared_sum[...]
        + jnp.dot(comb[0], returned[...], preferred_element_type=jnp.float32)
        + jnp.dot(comb[1], returned[...], preferred_element_type=jnp.float32)
    )
    for k in range(tp_count):
        cut_back[k] = combined[k * rows : (k + 1) * rows, :].astype(jnp.bfloat16)

    def send_fin(k, carry):
        other, device = tp_peer(k)
        pltpu.make_async_remote_copy(
            cut_back.at[other],
            landed.at[t],
            fin_send,
            fin_recv,
            device_id=device,
            device_id_type=MESH,
        ).start()
        return carry

    lax.fori_loop(1, tp_count, send_fin, 0)
    landed[t] = cut_back[t]

    most = tp_count - 1
    for ref, sem in (
        (pre.at[pl.ds(0, most)], pre_send),
        (mixes.at[pl.ds(0, most)], mix_send),
        (outgoing.at[pl.ds(0, 992)], go_send),
        (pooled.at[pl.ds(0, most)], ag_send),
        (partial.at[pl.ds(0, most)], rs_send),
        (result.at[pl.ds(0, 992)], back_send),
        (landed.at[pl.ds(0, most)], fin_recv),
        (landed.at[pl.ds(0, most)], fin_send),
    ):
        pltpu.make_async_copy(ref, ref, sem).wait()

    @pl.when(core == 0)
    def _():
        pair_copy(z).wait_send()

    for n in range(most_up):

        @pl.when(goes_up(n))
        def _():
            up_copy(n).wait_send()

    for n in range(most_down):

        @pl.when(goes_down(n))
        def _():
            down_copy(n).wait_send()

    for n in range(1, chips):

        @pl.when(z >= n)
        def _():
            pair_copy(z - n).wait_send()

    for k in range(tp_count):
        out[:, k * 128 : (k + 1) * 128] = landed[k]


def both_halves(
    queries,
    keys,
    values,
    key_bias,
    moe_in,
    norm_gain,
    route_ids,
    route_weights,
    gate_weight,
    up_weight,
    down_weight,
    shared_gate,
    shared_up,
    shared_down,
):
    own_rows, width = moe_in.shape
    tokens, head_dim = queries.shape
    bias_rows = key_bias.reshape(tokens // head_dim, head_dim)
    bias_rows = jnp.pad(bias_rows, ((0, 16 - tokens // head_dim), (0, 0)))
    hidden = gate_weight.shape[1]
    bf16, f32 = jnp.bfloat16, jnp.float32
    vmem, dma = pltpu.VMEM, pltpu.SemaphoreType.DMA
    here, there = pl.BlockSpec(memory_space=pltpu.VMEM), pl.BlockSpec(memory_space=pl.ANY)
    return pl.pallas_call(
        both_kernel,
        out_shape=(
            jax.ShapeDtypeStruct((tokens, head_dim), bf16),
            jax.ShapeDtypeStruct((own_rows, width), bf16),
        ),
        in_specs=[here] * 8 + [there] * 6,
        out_specs=(here, here),
        scratch_shapes=[
            vmem((32, 2 * tokens + 16, head_dim), bf16),
            vmem((2, 128, 128), f32),
            vmem((4, hidden, width), bf16),
            vmem((2, hidden, width), bf16),
            vmem((3, hidden, width), bf16),
            vmem((16, own_rows, 128), bf16),
            vmem((16, own_rows, 128), f32),
            vmem((16, own_rows, 128), bf16),
            vmem((1024, 128), bf16),
            vmem((16, 1152, 128), bf16),
            vmem((16, 1152, 128), bf16),
            vmem((4, 15, 288, 128), bf16),
            vmem((1152, 128), bf16),
            vmem((128, 128), f32),
            vmem((1024, 128), bf16),
            vmem((2, 128, 1024), bf16),
            vmem((16, own_rows, 128), bf16),
            vmem((16, own_rows, 128), bf16),
            dma((6,)),
            dma,
            dma,
            dma,
            dma,
            dma,
            dma,
            dma,
            dma((4, 16)),
            dma,
            dma((4, 15)),
            dma,
            dma,
            dma,
            dma,
            dma((8,)),
            dma((9,)),
            dma((8,)),
            dma((9,)),
            dma((16,)),
            dma((16,)),
            *attention_state(tokens, head_dim),
        ],
        compiler_params=pltpu.CompilerParams(
            collective_id=0, has_side_effects=True, vmem_limit_bytes=60 * 1024 * 1024
        ),
        cost_estimate=pl.CostEstimate(
            flops=80_000_000_000, bytes_accessed=200_000_000, transcendentals=300_000
        ),
    )(
        queries,
        keys,
        values,
        bias_rows,
        moe_in,
        norm_gain[None, :],
        route_ids.T,
        route_weights.T,
        gate_weight,
        up_weight,
        down_weight,
        shared_gate,
        shared_up,
        shared_down,
    )


def shards(
    queries,
    keys,
    values,
    key_bias,
    moe_in,
    norm_gain,
    route_ids,
    route_weights,
    gate_weight,
    up_weight,
    down_weight,
    shared_gate,
    shared_up,
    shared_down,
):
    return both_halves(
        queries,
        keys,
        values,
        key_bias,
        moe_in,
        norm_gain,
        route_ids,
        route_weights,
        gate_weight,
        up_weight,
        down_weight,
        shared_gate,
        shared_up,
        shared_down,
    )


def solution(mesh):
    split = Mesh(mesh.devices.reshape(mesh.shape["ep"], 4, 4), ("ep", "tp_0", "tp_1"))
    return jax.shard_map(
        shards,
        mesh=split,
        in_specs=(
            P("ep", TP),
            P("ep", TP),
            P("ep", TP),
            P("ep", TP),
            P(EP_TP, None),
            P(),
            P("ep", None),
            P(EP_TP, None),
            P("ep", TP, None),
            P("ep", TP, None),
            P("ep", TP, None),
            P(TP, None),
            P(TP, None),
            P(TP, None),
        ),
        out_specs=(P("ep", TP), P(EP_TP, None)),
        check_vma=False,
    )
```

```python
import functools

import jax
import jax.numpy as jnp
from jax import lax
from jax.experimental import pallas as pl
from jax.experimental.pallas import tpu as pltpu
from jax.sharding import Mesh
from jax.sharding import PartitionSpec as P

TP = ("tp_0", "tp_1")
EP_TP = ("ep", "tp_0", "tp_1")


norm_eps = 1e-05
MESH = pl.DeviceIdType.MESH


FAR = -1e30


def attention_start(state, row_count):
    scores_ref, logit_ref, sums_ref, soft_ref, weight_ref, tri, acc, later = state
    row_id = lax.broadcasted_iota(jnp.int32, tri.shape, 0)
    col_id = lax.broadcasted_iota(jnp.int32, tri.shape, 1)
    tri[...] = jnp.where((row_id > col_id) | (col_id >= 128), -1.0, 0.0).astype(jnp.bfloat16)
    acc[...] = jnp.zeros_like(acc)
    later[...] = jnp.zeros_like(later)
    sums_ref[...] = jnp.zeros_like(sums_ref)
    logit_ref[...] = jnp.full(logit_ref.shape, FAR, jnp.float32)
    scores_ref[...] = jnp.full(scores_ref.shape, FAR, jnp.float32)


def attention_finish_block(state, v_block):
    scores_ref, logit_ref, sums_ref, soft_ref, weight_ref, tri, acc, later = state
    num_rows = scores_ref.shape[0]
    piece = 16
    for first in range(0, num_rows, piece):
        carried = later[first : first + piece, :]
        for c in reversed(range(num_rows // 128)):
            at = c * num_rows + first
            weight_ref[first : first + piece, c * 128 : (c + 1) * 128] = jnp.exp(
                logit_ref[first : first + piece, c * 128 : (c + 1) * 128]
                + (sums_ref[at : at + piece, :128] + carried)
            ).astype(jnp.bfloat16)
            carried = carried + sums_ref[at : at + piece, 128:]
        later[first : first + piece, :] = carried
    acc[...] += jnp.dot(weight_ref[...], v_block, preferred_element_type=jnp.float32)


def attention_sum_block(state):
    scores_ref, logit_ref, sums_ref, soft_ref, weight_ref, tri, acc, later = state
    num_rows = scores_ref.shape[0]
    piece = 16
    for c in range(num_rows // 128):
        columns = slice(c * 128, (c + 1) * 128)
        for first in range(0, num_rows, piece):
            scores = scores_ref[first : first + piece, columns]
            soft = jnp.maximum(scores, jnp.log(1.0 + jnp.exp(jnp.minimum(scores, 88.0))))
            logit_ref[first : first + piece, columns] = scores - soft
            soft_ref[c * num_rows + first : c * num_rows + first + piece, :] = soft.astype(
                jnp.bfloat16
            )
    sums_ref[...] = jnp.dot(soft_ref[...], tri[...], preferred_element_type=jnp.float32)


def attention_score_block(state, q_ref, k_block, bias_rows, diagonal):
    scores_ref = state[0]
    num_rows, width = q_ref.shape
    bias = bias_rows.astype(jnp.float32)
    bias = jnp.concatenate([bias[r : r + 1] for r in range(num_rows // width)], axis=1)
    products = lax.dot_general(
        q_ref[...], k_block, (((1,), (1,)), ((), ())), preferred_element_type=jnp.float32
    )
    scores = products * width ** (-0.5) + bias
    if diagonal:
        causal = lax.broadcasted_iota(jnp.int32, scores.shape, 1) < lax.broadcasted_iota(
            jnp.int32, scores.shape, 0
        )
        scores = jnp.where(causal, scores, FAR)
    scores_ref[...] = scores


def attention_parts(kv_ref, block, num_rows):
    return (
        kv_ref[block, :num_rows, :],
        kv_ref[block, num_rows : 2 * num_rows, :],
        kv_ref[block, 2 * num_rows : 2 * num_rows + 16, :],
    )


def attention_step(state, q_ref, kv_ref, me, count):
    num_rows = q_ref.shape[0]
    v_block = attention_parts(kv_ref, jnp.minimum(me - count + 2, me), num_rows)[1]
    k_block, _, bias_rows = attention_parts(kv_ref, jnp.maximum(me - count, 0), num_rows)
    attention_finish_block(state, v_block)
    attention_sum_block(state)
    attention_score_block(state, q_ref, k_block, bias_rows, False)


def attention_end(state, o_ref):
    raw_out = state[6][...]
    o_ref[...] = (
        raw_out * lax.rsqrt(jnp.mean(raw_out * raw_out, axis=1, keepdims=True) + norm_eps)
    ).astype(jnp.bfloat16)


def attention_state(num_rows, width):
    f32, bf16 = jnp.float32, jnp.bfloat16
    pieces = num_rows // 128
    return [
        pltpu.VMEM((num_rows, num_rows), f32),
        pltpu.VMEM((num_rows, num_rows), f32),
        pltpu.VMEM((pieces * num_rows, 256), f32),
        pltpu.VMEM((pieces * num_rows, 128), bf16),
        pltpu.VMEM((num_rows, num_rows), bf16),
        pltpu.VMEM((128, 256), bf16),
        pltpu.VMEM((num_rows, width), f32),
        pltpu.VMEM((num_rows, 128), f32),
    ]


def both_kernel(
    queries,
    keys,
    values,
    bias_rows,
    moe_in,
    gain,
    ids_across,
    mix_across,
    gate,
    up,
    down,
    shared_gate,
    shared_up,
    shared_down,
    heads,
    out,
    kv,
    turned,
    w_in,
    w_out,
    w_shared,
    cut,
    mixes,
    pre,
    outgoing,
    pooled,
    partial,
    inbox,
    result,
    shared_sum,
    returned,
    comb,
    cut_back,
    landed,
    w_sem,
    pre_send,
    pre_recv,
    mix_send,
    mix_recv,
    go_send,
    go_recv,
    ag_send,
    ag_recv,
    rs_send,
    rs_recv,
    back_send,
    back_recv,
    fin_send,
    fin_recv,
    up_send,
    up_recv,
    down_send,
    down_recv,
    pair_send,
    pair_recv,
    *state,
):
    ep_count, tp_count = lax.axis_size("ep"), 16
    rows = moe_in.shape[0]
    e = lax.axis_index("ep")
    y = lax.axis_index("tp_0")
    x = lax.axis_index("tp_1")
    t = y * 4 + x

    def tp_peer(k):
        other = lax.rem(t + k, tp_count)
        return other, {"tp_0": other // 4, "tp_1": lax.rem(other, 4)}

    barrier = pltpu.get_barrier_semaphore()

    def greet_tp(k, carry):
        pl.semaphore_signal(barrier, inc=1, device_id=tp_peer(k)[1], device_id_type=MESH)
        return carry

    def greet_ep(k, carry):
        pl.semaphore_signal(
            barrier, inc=1, device_id={"ep": lax.rem(e + k, ep_count)}, device_id_type=MESH
        )
        return carry

    lax.fori_loop(1, ep_count, greet_ep, 0)
    lax.fori_loop(1, tp_count, greet_tp, 0)

    loads = [
        pltpu.make_async_copy(gate, w_in.at[pl.ds(0, 2)], w_sem.at[0]),
        pltpu.make_async_copy(up, w_in.at[pl.ds(2, 2)], w_sem.at[1]),
        pltpu.make_async_copy(down, w_out, w_sem.at[2]),
        pltpu.make_async_copy(shared_gate, w_shared.at[0], w_sem.at[3]),
        pltpu.make_async_copy(shared_up, w_shared.at[1], w_sem.at[4]),
        pltpu.make_async_copy(shared_down, w_shared.at[2], w_sem.at[5]),
    ]
    for load in loads:
        load.start()

    as_float = moe_in[...].astype(jnp.float32)
    normed = (
        as_float
        * lax.rsqrt(jnp.mean(as_float * as_float, axis=1, keepdims=True) + norm_eps)
        * gain[...]
    ).astype(jnp.bfloat16)
    for k in range(tp_count):
        cut[k] = normed[:, k * 128 : (k + 1) * 128]
    top_k = ids_across.shape[0]
    turned[...] = jnp.zeros_like(turned)
    turned[0, :top_k, :] = ids_across[...].astype(jnp.float32)
    turned[1, :top_k, :rows] = mix_across[...]
    own_mix = turned[1].T[:rows, :]
    turned[0] = turned[0].T
    own_ids = turned[0, pl.ds(pl.multiple_of(t * rows, rows), rows), :]
    lane = lax.broadcasted_iota(jnp.int32, (rows, 128), 1).astype(jnp.float32)
    spread = jnp.zeros((rows, 128), jnp.float32)
    for k in range(top_k):
        spread = spread + jnp.where(own_ids[:, k : k + 1] == lane, own_mix[:, k : k + 1], 0.0)
    mixes[t] = spread
    pre[t] = cut[t]

    tokens = queries.shape[0]
    kv[e, :tokens, :] = keys[...]
    kv[e, tokens : 2 * tokens, :] = values[...]
    kv[e, 2 * tokens : 2 * tokens + 16, :] = bias_rows[...]
    attention_start(state, tokens)

    pl.semaphore_wait(barrier, ep_count + tp_count - 2)

    chips = ep_count // 2
    z, core = e // 2, lax.rem(e, 2)
    partner = e + 1 - 2 * core
    most_up, most_down = chips // 2, chips // 2 - 1

    def kv_copy(chip, target, send_sem, recv_sem):
        ref = kv.at[chip * 2 + core]
        return pltpu.make_async_remote_copy(
            ref, ref, send_sem, recv_sem, device_id={"ep": target}, device_id_type=MESH
        )

    def chip_at(step):
        return lax.rem(z + step + chips, chips)

    def up_copy(n):
        return kv_copy(
            chip_at(-n), chip_at(1) * 2 + core, up_send.at[n], up_recv.at[n + 1]
        )

    def down_copy(n):
        return kv_copy(
            chip_at(n), chip_at(-1) * 2 + core, down_send.at[n], down_recv.at[n + 1]
        )

    def pair_copy(chip):
        return kv_copy(chip, partner, pair_send.at[chip], pair_recv.at[chip])

    def goes_up(n):
        return (z - n >= 0) & (z < chips - 1)

    def goes_down(n):
        return chip_at(n) < most_down

    def kv_service(n):
        @pl.when(z >= n)
        def _():
            up_copy(n - 1).wait_recv()
            pair_copy(z - n).start()

        if n < most_up:

            @pl.when(goes_up(n))
            def _():
                up_copy(n).start()

        if n <= most_down:

            @pl.when(goes_down(n))
            def _():
                down_copy(n - 1).wait_recv()

                @pl.when(chip_at(n) < z)
                def _():
                    pair_copy(chip_at(n)).start()

                if n < most_down:
                    down_copy(n).start()

    def attend(first, last):
        def pair(n, carry):
            @pl.when(z >= n)
            def _():
                pair_wait(z - n)
                for extra in range(2):
                    attention_step(state, queries, kv, e, 2 * n - 1 + core + extra)

            return carry

        lax.fori_loop(first, last + 1, pair, 0)

    def pair_wait(chip):
        ref = kv.at[chip * 2 + 1 - core]
        pltpu.make_async_copy(ref, ref, pair_recv.at[chip]).wait()


    def send_pre(k, carry):
        other, device = tp_peer(k)
        pltpu.make_async_remote_copy(
            cut.at[other], pre.at[t], pre_send, pre_recv, device_id=device, device_id_type=MESH
        ).start()
        return carry

    def send_mix(k, carry):
        _, device = tp_peer(k)
        pltpu.make_async_remote_copy(
            mixes.at[t], mixes.at[t], mix_send, mix_recv, device_id=device, device_id_type=MESH
        ).start()
        return carry

    lax.fori_loop(1, tp_count, send_pre, 0)

    @pl.when(core == 0)
    def _():
        pair_copy(z).start()

    @pl.when(goes_up(0))
    def _():
        up_copy(0).start()

    @pl.when(goes_down(0))
    def _():
        down_copy(0).start()


    across = ids_across[...]
    expert_id = lax.broadcasted_iota(jnp.int32, (64, 128), 0)
    named = across[0:1] == expert_id
    for k in range(1, across.shape[0]):
        named = named | (across[k : k + 1] == expert_id)
    named = named.astype(jnp.float32)
    source = lax.broadcasted_iota(jnp.int32, (tp_count, 128), 0)
    same = (lax.broadcasted_iota(jnp.int32, (tp_count, 128), 1) // rows == source).astype(
        jnp.float32
    )
    for k in range(64):
        outgoing[k * 16 : (k + 1) * 16, :] = (same * named[k : k + 1, :]).astype(jnp.bfloat16)

    pltpu.make_async_copy(
        pre.at[pl.ds(0, tp_count - 1)], pre.at[pl.ds(0, tp_count - 1)], pre_recv
    ).wait()
    own_rows = pre[...].astype(jnp.float32).reshape(tp_count * rows, 128).astype(jnp.bfloat16)
    pooled[t, 1024:1152, :] = own_rows
    for k in range(4):
        part = slice(k * 256, (k + 1) * 256)
        outgoing[part, :] = jnp.dot(
            outgoing[part, :], own_rows, preferred_element_type=jnp.float32
        ).astype(jnp.bfloat16)
    at_e = pl.ds(pl.multiple_of(e * 32, 32), 32)

    def send_go(k, carry):
        other = lax.rem(e + k, ep_count)
        pltpu.make_async_remote_copy(
            outgoing.at[pl.ds(pl.multiple_of(other * 32, 32), 32)],
            pooled.at[t, at_e],
            go_send,
            go_recv,
            device_id={"ep": other},
            device_id_type=MESH,
        ).start()
        return carry

    lax.fori_loop(1, ep_count, send_go, 0)
    lax.fori_loop(1, tp_count, send_mix, 0)
    pooled[t, at_e, :] = outgoing[at_e, :]
    kv_service(1)
    k_block, _, own_bias = attention_parts(kv, e, tokens)
    attention_score_block(state, queries, k_block, own_bias, True)

    @pl.when(core == 1)
    def _():
        pair_wait(z)
        attention_step(state, queries, kv, e, 1)

    attend(1, 1)

    pltpu.make_async_copy(
        mixes.at[pl.ds(0, tp_count - 1)], mixes.at[pl.ds(0, tp_count - 1)], mix_recv
    ).wait()
    mix_all = mixes[...].reshape(tp_count * rows, 128)
    high = mix_all.astype(jnp.bfloat16)
    low = (mix_all - high.astype(jnp.float32)).astype(jnp.bfloat16)
    for k in range(4):
        column = k * 256 + lax.broadcasted_iota(jnp.int32, (128, 256), 1)
        row = lax.broadcasted_iota(jnp.int32, (128, 256), 0)
        widen = (column // 16 == row).astype(jnp.bfloat16)
        keep = lax.rem(column, 16) == row // rows
        for part, value in ((0, high), (1, low)):
            wide = jnp.dot(value, widen, preferred_element_type=jnp.float32)
            comb[part, :, k * 256 : (k + 1) * 256] = jnp.where(keep, wide, 0.0).astype(
                jnp.bfloat16
            )

    pltpu.make_async_copy(
        pooled.at[t, pl.ds(0, 992)], pooled.at[t, pl.ds(0, 992)], go_recv
    ).wait()

    quarter = 288
    names = ("tp_0", "tp_1")
    place = {"tp_0": y, "tp_1": x}

    def axes(q):
        first, second = names if q < 2 else names[::-1]
        return first, second, 1 if q % 2 == 0 else 3

    def index_at(q, df, dg):
        first, second, _ = axes(q)
        moved = {
            first: lax.rem(place[first] + df % 4, 4),
            second: lax.rem(place[second] + dg % 4, 4),
        }
        return moved["tp_0"] * 4 + moved["tp_1"]

    def block(ref, q, df, dg):
        return ref.at[index_at(q, df, dg), pl.ds(q * quarter, quarter)]

    def ag_copy(q, df, dg, along_first, step):
        first, second, _ = axes(q)
        axis = first if along_first else second
        there = ((df - step) % 4, dg % 4) if along_first else (df % 4, (dg - step) % 4)
        ref = block(pooled, q, df, dg)
        return pltpu.make_async_remote_copy(
            ref,
            ref,
            ag_send,
            ag_recv.at[q, there[0] * 4 + there[1]],
            device_id={axis: lax.rem(place[axis] + step % 4, 4)},
            device_id_type=MESH,
        )

    def ag_wait(q, df, dg):
        ref = block(pooled, q, df, dg)
        pltpu.make_async_copy(ref, ref, ag_recv.at[q, (df % 4) * 4 + dg % 4]).wait()

    quarters = range(4)
    for q in quarters:
        ag_copy(q, 0, 0, True, 1).start()
        ag_copy(q, 0, 0, True, 3).start()
    for q in quarters:
        ag_copy(q, 0, 0, False, 1).start()
        ag_copy(q, 0, 0, False, 3).start()
    for q in quarters:
        d = axes(q)[2]
        ag_wait(q, -d, 0)
        ag_copy(q, -d, 0, True, d).start()
        ag_copy(q, -d, 0, False, 1).start()
        ag_copy(q, -d, 0, False, 3).start()
    kv_service(2)
    for q in quarters:
        d = axes(q)[2]
        ag_wait(q, d, 0)
        ag_copy(q, d, 0, False, 1).start()
        ag_copy(q, d, 0, False, 3).start()
    for q in quarters:
        d = axes(q)[2]
        ag_wait(q, 0, -d)
        ag_copy(q, 0, -d, False, d).start()
    for q in quarters:
        ag_wait(q, 2, 0)
        ag_copy(q, 2, 0, False, 1).start()
        ag_copy(q, 2, 0, False, 3).start()
        if q == 1:
            kv_service(3)
    for hop in range(3):
        for q in quarters:
            d = axes(q)[2]
            df = (-d, d, 2)[hop]
            ag_wait(q, df, -d)
            ag_copy(q, df, -d, False, d).start()
            if hop == 1 and q == 1:
                kv_service(4)
    attend(2, 2)
    kv_service(5)
    attend(3, 3)

    for load in loads:
        load.wait()

    def rs_copy(q, ref, slot, along_first, step):
        first, second, _ = axes(q)
        axis = first if along_first else second
        return pltpu.make_async_remote_copy(
            ref,
            inbox.at[q, slot],
            rs_send,
            rs_recv.at[q, slot],
            device_id={axis: lax.rem(place[axis] + step % 4, 4)},
            device_id_type=MESH,
        )

    def rs_wait(q, slot):
        ref = inbox.at[q, slot]
        pltpu.make_async_copy(ref, ref, rs_recv.at[q, slot]).wait()

    def plus(q, df, dg, *slots):
        where = index_at(q, df, dg)
        total = partial[where, q * quarter : (q + 1) * quarter, :].astype(jnp.float32)
        for slot in slots:
            total = total + inbox[q, slot].astype(jnp.float32)
        return where, total

    def silu_times(both):
        half = both.shape[1] // 2
        gate_val = both[:, :half]
        return gate_val * (1.0 / (1.0 + jnp.exp(-gate_val))) * both[:, half:]

    def feed(span, weights_in, weights_out, routed):
        both = jnp.concatenate([pooled[k, span, :] for k in range(tp_count)], axis=1)
        hidden = silu_times(
            lax.dot_general(
                both, weights_in, (((1,), (1,)), ((), ())), preferred_element_type=jnp.float32
            )
        )
        if routed:
            row = lax.broadcasted_iota(jnp.int32, hidden.shape, 0)
            column = lax.broadcasted_iota(jnp.int32, hidden.shape, 1)
            hidden = jnp.where(lax.rem(row // 16, 2) == column // 64, hidden, 0.0)
        hidden = hidden.astype(jnp.bfloat16)
        for k in range(0, tp_count, 2):
            term = jnp.dot(
                hidden,
                weights_out[:, k * 128 : (k + 2) * 128],
                preferred_element_type=jnp.float32,
            ).astype(jnp.bfloat16)
            partial[k, span, :] = term[:, :128]
            partial[k + 1, span, :] = term[:, 128:]

    for q in quarters:
        d = axes(q)[2]
        for df in range(4):
            ag_wait(q, df, d)
            ag_wait(q, df, 2)
        last = q == 3
        span = slice(q * quarter, 1024 if last else (q + 1) * quarter)
        feed(span, w_in[...].reshape(256, 2048), w_out[...].reshape(128, 2048), True)
        if last:
            feed(
                slice(1024, 1152), w_shared[0:2].reshape(128, 2048), w_shared[2], False
            )
        for df in (2, -d, d, 0):
            slot = (df % 4) * 3
            rs_copy(q, block(partial, q, df, 2), slot, False, d).start()
            rs_copy(q, block(partial, q, df, -d), slot + 1, False, -d).start()
        if q == 1:
            kv_service(6)

    attend(4, 5)
    kv_service(7)
    rows_of = lambda q: slice(q * quarter, (q + 1) * quarter)
    for turn in range(4):
        for q in quarters:
            d = axes(q)[2]
            df = (2, -d, d, 0)[turn] % 4
            rs_wait(q, df * 3)
            where, total = plus(q, df, d, df * 3)
            partial[where, rows_of(q), :] = total.astype(jnp.bfloat16)
            rs_copy(q, block(partial, q, df, d), df * 3 + 2, False, d).start()
        attend(turn + 6, turn + 6)
        if turn == 1:
            kv_service(8)
    for turn in range(4):
        for q in quarters:
            d = axes(q)[2]
            df = (2, -d, d, 0)[turn] % 4
            rs_wait(q, df * 3 + 1)
            rs_wait(q, df * 3 + 2)
            slots = [df * 3 + 1, df * 3 + 2]
            if turn == 2:
                rs_wait(q, 12)
                slots.append(12)
            where, total = plus(q, df, 0, *slots)
            partial[where, rows_of(q), :] = total.astype(jnp.bfloat16)
            if turn == 0:
                rs_copy(q, block(partial, q, df, 0), 12, True, d).start()
            elif turn == 1:
                rs_copy(q, block(partial, q, df, 0), 13, True, -d).start()
            elif turn == 2:
                rs_copy(q, block(partial, q, df, 0), 14, True, d).start()
        if turn < 3:
            attend(turn + 10, turn + 10)

    for q in quarters:
        rs_wait(q, 13)
        rs_wait(q, 14)
        _, total = plus(q, 0, 0, 13, 14)
        result[rows_of(q), :] = total.astype(jnp.bfloat16)
        if q == 3:
            shared_sum[...] = total[160:288, :]

        def send_back(other, carry):
            @pl.when(other != e)
            def _():
                pltpu.make_async_remote_copy(
                    result.at[pl.ds(pl.multiple_of(other * 32, 32), 32)],
                    returned.at[at_e],
                    back_send,
                    back_recv,
                    device_id={"ep": other},
                    device_id_type=MESH,
                ).start()

            return carry

        lax.fori_loop(q * 9, min(ep_count, (q + 1) * 9), send_back, 0)
    returned[at_e, :] = result[at_e, :]
    attend(13, chips - 1)
    for extra in range(2):
        attention_step(state, queries, kv, e, e + 1 + extra)
    attention_end(state, heads)
    pltpu.make_async_copy(
        returned.at[pl.ds(0, 992)], returned.at[pl.ds(0, 992)], back_recv
    ).wait()
    combined = (
        shared_sum[...]
        + jnp.dot(comb[0], returned[...], preferred_element_type=jnp.float32)
        + jnp.dot(comb[1], returned[...], preferred_element_type=jnp.float32)
    )
    for k in range(tp_count):
        cut_back[k] = combined[k * rows : (k + 1) * rows, :].astype(jnp.bfloat16)

    def send_fin(k, carry):
        other, device = tp_peer(k)
        pltpu.make_async_remote_copy(
            cut_back.at[other],
            landed.at[t],
            fin_send,
            fin_recv,
            device_id=device,
            device_id_type=MESH,
        ).start()
        return carry

    lax.fori_loop(1, tp_count, send_fin, 0)
    landed[t] = cut_back[t]

    most = tp_count - 1
    for ref, sem in (
        (pre.at[pl.ds(0, most)], pre_send),
        (mixes.at[pl.ds(0, most)], mix_send),
        (outgoing.at[pl.ds(0, 992)], go_send),
        (pooled.at[pl.ds(0, most)], ag_send),
        (partial.at[pl.ds(0, most)], rs_send),
        (result.at[pl.ds(0, 992)], back_send),
        (landed.at[pl.ds(0, most)], fin_recv),
        (landed.at[pl.ds(0, most)], fin_send),
    ):
        pltpu.make_async_copy(ref, ref, sem).wait()

    @pl.when(core == 0)
    def _():
        pair_copy(z).wait_send()

    for n in range(most_up):

        @pl.when(goes_up(n))
        def _():
            up_copy(n).wait_send()

    for n in range(most_down):

        @pl.when(goes_down(n))
        def _():
            down_copy(n).wait_send()

    for n in range(1, chips):

        @pl.when(z >= n)
        def _():
            pair_copy(z - n).wait_send()

    for k in range(tp_count):
        out[:, k * 128 : (k + 1) * 128] = landed[k]


def both_halves(
    queries,
    keys,
    values,
    key_bias,
    moe_in,
    norm_gain,
    route_ids,
    route_weights,
    gate_weight,
    up_weight,
    down_weight,
    shared_gate,
    shared_up,
    shared_down,
):
    own_rows, width = moe_in.shape
    tokens, head_dim = queries.shape
    bias_rows = key_bias.reshape(tokens // head_dim, head_dim)
    bias_rows = jnp.pad(bias_rows, ((0, 16 - tokens // head_dim), (0, 0)))
    hidden = gate_weight.shape[1]
    bf16, f32 = jnp.bfloat16, jnp.float32
    vmem, dma = pltpu.VMEM, pltpu.SemaphoreType.DMA
    here, there = pl.BlockSpec(memory_space=pltpu.VMEM), pl.BlockSpec(memory_space=pl.ANY)
    return pl.pallas_call(
        both_kernel,
        out_shape=(
            jax.ShapeDtypeStruct((tokens, head_dim), bf16),
            jax.ShapeDtypeStruct((own_rows, width), bf16),
        ),
        in_specs=[here] * 8 + [there] * 6,
        out_specs=(here, here),
        scratch_shapes=[
            vmem((32, 2 * tokens + 16, head_dim), bf16),
            vmem((2, 128, 128), f32),
            vmem((4, hidden, width), bf16),
            vmem((2, hidden, width), bf16),
            vmem((3, hidden, width), bf16),
            vmem((16, own_rows, 128), bf16),
            vmem((16, own_rows, 128), f32),
            vmem((16, own_rows, 128), bf16),
            vmem((1024, 128), bf16),
            vmem((16, 1152, 128), bf16),
            vmem((16, 1152, 128), bf16),
            vmem((4, 15, 288, 128), bf16),
            vmem((1152, 128), bf16),
            vmem((128, 128), f32),
            vmem((1024, 128), bf16),
            vmem((2, 128, 1024), bf16),
            vmem((16, own_rows, 128), bf16),
            vmem((16, own_rows, 128), bf16),
            dma((6,)),
            dma,
            dma,
            dma,
            dma,
            dma,
            dma,
            dma,
            dma((4, 16)),
            dma,
            dma((4, 15)),
            dma,
            dma,
            dma,
            dma,
            dma((8,)),
            dma((9,)),
            dma((8,)),
            dma((9,)),
            dma((16,)),
            dma((16,)),
            *attention_state(tokens, head_dim),
        ],
        compiler_params=pltpu.CompilerParams(
            collective_id=0, has_side_effects=True, vmem_limit_bytes=60 * 1024 * 1024
        ),
        cost_estimate=pl.CostEstimate(
            flops=80_000_000_000, bytes_accessed=200_000_000, transcendentals=300_000
        ),
    )(
        queries,
        keys,
        values,
        bias_rows,
        moe_in,
        norm_gain[None, :],
        route_ids.T,
        route_weights.T,
        gate_weight,
        up_weight,
        down_weight,
        shared_gate,
        shared_up,
        shared_down,
    )


def shards(
    queries,
    keys,
    values,
    key_bias,
    moe_in,
    norm_gain,
    route_ids,
    route_weights,
    gate_weight,
    up_weight,
    down_weight,
    shared_gate,
    shared_up,
    shared_down,
):
    return both_halves(
        queries,
        keys,
        values,
        key_bias,
        moe_in,
        norm_gain,
        route_ids,
        route_weights,
        gate_weight,
        up_weight,
        down_weight,
        shared_gate,
        shared_up,
        shared_down,
    )


def solution(mesh):
    split = Mesh(mesh.devices.reshape(mesh.shape["ep"], 4, 4), ("ep", "tp_0", "tp_1"))
    return jax.shard_map(
        shards,
        mesh=split,
        in_specs=(
            P("ep", TP),
            P("ep", TP),
            P("ep", TP),
            P("ep", TP),
            P(EP_TP, None),
            P(),
            P("ep", None),
            P(EP_TP, None),
            P("ep", TP, None),
            P("ep", TP, None),
            P("ep", TP, None),
            P(TP, None),
            P(TP, None),
            P(TP, None),
        ),
        out_specs=(P("ep", TP), P(EP_TP, None)),
        check_vma=False,
    )
```
